512 devices in a mesh: ep: 32 (over z, core), tp: 16 (over y, x).
Axes of the slice: x: 4, y: 4, z: 16, core: 2. Of those that a mesh axis runs over, the one named last changes fastest.
Arguments:
- tokens: bfloat16 [4096, 2048], P('ep'), may hold values from -6 to 6
- routes: int32 [4096, 2], P('ep'), may hold values from 0 to 15, all different within a row; in each aligned block of 128 rows (0 to 127, 128 to 255, ...) at most 18 rows name the same one
- route_weights: float32 [4096, 2], P('ep'), may hold values from 0.2 to 1
- out_grad: bfloat16 [4096, 2048], P('ep'), may hold values from -6 to 6
- gate_proj: bfloat16 [32, 2048, 2048], P('ep', None, 'tp'), may hold values from -0.125 to 0.125
- up_proj: bfloat16 [32, 2048, 2048], P('ep', None, 'tp'), may hold values from -0.125 to 0.125
- down_proj: bfloat16 [32, 2048, 2048], P('ep', 'tp'), may hold values from -0.09375 to 0.09375
Outputs:
- tokens_grad: bfloat16 [4096, 2048], P('ep', 'tp')
- route_grad: float32 [4096, 2], P('ep')
- gate_grad: bfloat16 [32, 2048, 2048], P('ep', None, 'tp')
- up_grad: bfloat16 [32, 2048, 2048], P('ep', None, 'tp')
- down_grad: bfloat16 [32, 2048, 2048], P('ep', 'tp')
The draws below stay inside these ranges and needn't reach their ends.
Inputs may be any that keep to these rules, and one draw needn't show every extreme that they name: `routes`: each row names 2 different experts. In the rows of one device (an aligned block of 128 rows) no expert is named more than 18 times, and in some blocks one expert is named exactly 18 times.
All inputs are finite; a program needn't handle non-finite values.
Results may differ from the reference program's by a relative error of at most 0.019.
Values may be sent and summed in bfloat16 or wider, within the bound.
No kernel may reach another device: no remote copies, remote signals or barrier semaphores. Data moves between devices by JAX's collectives and lax.ppermute only.
A program may use at most 64 MiB of HBM per device.

```python
import math
import jax
import jax.numpy as jnp
import numpy as np
from jax import lax

D = 2048
FF = 4096
TOP = 2
TOK_DEV = 128
EXPERTS = 16
SOURCES = 32
GROUPS = 16
HALF = 2048
CAP = 18
ROWS = 576
TOKENS = 4096


def steps_of(rng, shape, pieces, low, largest):
    factor_of, own = 1.0, jax.random.fold_in(rng, 6)
    for dim, blocks in pieces:
        draws = jnp.exp(jax.random.uniform(jax.random.fold_in(own, dim), (blocks,), jnp.float32, low / len(pieces), largest / len(pieces)))
        factor_of = factor_of * jnp.repeat(draws, shape[dim] // blocks).reshape([-1 if axis == dim else 1 for axis in range(len(shape))])
    return factor_of


def shared_out(key, own, number, rows, number_of, top, limit, lean):
    ranking = jax.random.permutation(key, number_of)
    crowded, ordinary = portions_of(number_of, rows * top, limit, lean, True), portions_of(number_of, rows * top, limit, lean, False)
    places = jnp.arange(number_of)

    def named(tallies, rotation):
        used = int((tallies > 0).sum())
        fixed = max(1, used // 4)
        passed = fixed + (places - fixed + rotation * (used - fixed)) % max(1, number_of - fixed)
        return jnp.zeros((number_of,), jnp.int32).at[ranking[jnp.where(places < fixed, places, passed)]].set(jnp.asarray(tallies, jnp.int32))

    tallies = jnp.where(number % 4 == 0, named(crowded, number // 4), named(ordinary, number - number // 4 - 1))
    mixed = jax.random.permutation(jax.random.fold_in(own, 3), number_of)
    source_of, taker = mixed[0:number_of // 2 * 2:2], mixed[1:number_of // 2 * 2:2]
    slack = jnp.minimum(tallies[source_of] - 1, limit - tallies[taker]) // 2
    slack = jnp.where((source_of == ranking[0]) | (taker == ranking[0]) | (tallies[taker] == 0), 0, jnp.maximum(slack, 0))
    passed = jax.random.randint(jax.random.fold_in(own, 4), (number_of // 2,), 0, 1 << 20) % (slack + 1)
    tallies = tallies.at[source_of].add(-passed).at[taker].add(passed)
    members = jnp.searchsorted(jnp.cumsum(tallies), jnp.arange(rows * top), side="right").astype(jnp.int32)
    listing = members.reshape(top, rows).T
    listing = listing[jax.random.permutation(jax.random.fold_in(own, 1), rows)]
    rotation = jax.random.randint(jax.random.fold_in(own, 2), (rows, 1), 0, top)
    return jnp.take_along_axis(listing, (jnp.arange(top)[None, :] + rotation) % top, axis=1)


def portions_of(number_of, total, most, lean, full):
    portions = [(1 << 20) // math.isqrt(standing ** lean) + 1 for standing in range(1, number_of + 1)]
    largest = most if full else min(most, max(-(-total // number_of), total * portions[0] // sum(portions)))
    least = 1 if total - largest >= number_of - 1 else 0
    holding, rest = [largest] + [least] * (number_of - 1), total - largest - least * (number_of - 1)
    while rest > 0:
        free = [i for i in range(1, number_of) if holding[i] < largest] or [i for i in range(1, number_of) if holding[i] < most]
        whole, remaining = sum([portions[i] for i in free]), rest
        for i in free:
            more = min(most - holding[i], max(1, remaining * portions[i] // whole), rest)
            holding[i] = holding[i] + more
            rest = rest - more
    return np.array(holding)


def gaussian(rng, extent, spread, most, split=(), kind=jnp.bfloat16):
    array = spread * jax.random.normal(rng, extent, jnp.float32)
    if split:
        array = array * steps_of(rng, extent, split, -0.22, 0.18)
    return jnp.clip(array, -most, most).astype(kind)


def setup_inputs(seed: int = 0) -> dict:
    seeds = jax.random.split(jax.random.key(seed), 8)
    tokens = gaussian(seeds[0], (TOKENS, D), 1.0, 6.0, ((0, 32),))
    routes_keys = jax.random.split(jax.random.fold_in(seeds[1], 1), TOKENS // TOK_DEV)
    routes_turns = jax.random.permutation(jax.random.fold_in(seeds[1], 3), TOKENS // TOK_DEV)
    routes = jax.vmap(lambda own, number: shared_out(jax.random.fold_in(seeds[1], 2), own, number, TOK_DEV, EXPERTS, TOP, CAP, 2))(routes_keys, routes_turns).reshape((TOKENS, TOP))
    route_weights = jnp.clip(0.2 + 0.8 * jax.random.uniform(seeds[2], (TOKENS, TOP), jnp.float32) ** steps_of(seeds[2], (TOKENS, TOP), ((0, 32),), -0.2, 0.2), 0.2, 1.0)
    out_grad = gaussian(seeds[3], (TOKENS, D), 1.0, 6.0, ((0, 32),))
    gate_proj = gaussian(seeds[4], (2 * EXPERTS, D, HALF), D ** -0.5, 0.125, ((0, 32), (2, 16)))
    up_proj = gaussian(seeds[5], (2 * EXPERTS, D, HALF), D ** -0.5, 0.125, ((0, 32), (2, 16)))
    down_proj = gaussian(seeds[6], (2 * EXPERTS, HALF, D), FF ** -0.5, 0.09375, ((0, 32), (1, 16)))
    return dict(tokens=tokens, routes=routes, route_weights=route_weights, out_grad=out_grad, gate_proj=gate_proj, up_proj=up_proj, down_proj=down_proj)


def slot_rows(routes):
    blocks = routes.reshape(SOURCES, TOK_DEV * TOP)
    one_hot = (blocks[:, :, None] == jnp.arange(EXPERTS, dtype=jnp.int32)[None, None, :]).astype(jnp.int32)
    earlier = jnp.cumsum(one_hot, axis=1) - one_hot
    slot_index = jnp.sum(earlier * one_hot, axis=2)
    source = jnp.arange(SOURCES, dtype=jnp.int32)[:, None]
    return (blocks * ROWS + source * CAP + slot_index).reshape(-1).astype(jnp.int32)


def contract_rows(left, right):
    return lax.dot_general(left, right, (((0,), (0,)), ((), ())), preferred_element_type=jnp.float32)


def reference(tokens, routes, route_weights, out_grad, gate_proj, up_proj, down_proj):
    position = slot_rows(routes)
    owner = (jnp.arange(TOKENS * TOP, dtype=jnp.int32) // TOP).astype(jnp.int32)
    all_rows = EXPERTS * ROWS
    x_all = jnp.zeros((all_rows, D), jnp.bfloat16).at[position].set(tokens[owner]).reshape(EXPERTS, ROWS, D)
    dy_all = jnp.zeros((all_rows, D), jnp.bfloat16).at[position].set(out_grad[owner]).reshape(EXPERTS, ROWS, D)
    g_all = jnp.zeros((all_rows,), jnp.float32).at[position].set(route_weights.reshape(-1)).reshape(EXPERTS, ROWS)
    group_width = HALF // GROUPS

    def one_half(index):
        expert = index // 2
        x_rows = x_all[expert]
        dy_rows = dy_all[expert]
        g_rows = g_all[expert][:, None]
        gate_w = gate_proj[index]
        up_w = up_proj[index]
        down_w = down_proj[index]
        pre_gate = jnp.dot(x_rows, gate_w, preferred_element_type=jnp.float32)
        pre_up = jnp.dot(x_rows, up_w, preferred_element_type=jnp.float32)
        sigma = jax.nn.sigmoid(pre_gate)
        activ = pre_gate * sigma
        hidden = activ * pre_up
        d_hidden = lax.dot_general(dy_rows, down_w, (((1,), (1,)), ((), ())), preferred_element_type=jnp.float32)
        gate_part = jnp.sum(hidden * d_hidden, axis=1)
        scaled = g_rows * d_hidden
        d_gate = (scaled * pre_up * sigma * (1.0 + pre_gate * (1.0 - sigma))).astype(jnp.bfloat16)
        d_up = (scaled * activ).astype(jnp.bfloat16)
        scaled_cot = (g_rows * dy_rows.astype(jnp.float32)).astype(jnp.bfloat16)
        grad_gate = contract_rows(x_rows, d_gate).astype(jnp.bfloat16)
        grad_up = contract_rows(x_rows, d_up).astype(jnp.bfloat16)
        grad_down = contract_rows(hidden.astype(jnp.bfloat16), scaled_cot).astype(jnp.bfloat16)
        gate_three = d_gate.astype(jnp.float32).reshape(ROWS, GROUPS, group_width)
        up_three = d_up.astype(jnp.float32).reshape(ROWS, GROUPS, group_width)
        gate_wide = gate_w.astype(jnp.float32).reshape(D, GROUPS, group_width)
        up_wide = up_w.astype(jnp.float32).reshape(D, GROUPS, group_width)
        partial_value = jnp.einsum("rqc,dqc->qrd", gate_three, gate_wide, precision=lax.Precision.HIGHEST)
        partial_value = partial_value + jnp.einsum("rqc,dqc->qrd", up_three, up_wide, precision=lax.Precision.HIGHEST)
        rounded = lax.optimization_barrier(partial_value.astype(jnp.bfloat16)).astype(jnp.float32)
        row_grad = jnp.sum(rounded, axis=0).astype(jnp.bfloat16)
        return row_grad, gate_part, grad_gate, grad_up, grad_down

    row_grad, gate_part, gate_grad, up_grad, down_grad = lax.map(one_half, jnp.arange(2 * EXPERTS, dtype=jnp.int32))
    expert_rows = row_grad.astype(jnp.float32).reshape(EXPERTS, 2, ROWS, D).sum(axis=1).reshape(all_rows, D)
    expert_gate = gate_part.reshape(EXPERTS, 2, ROWS).sum(axis=1).reshape(all_rows)
    tokens_grad = expert_rows[position].reshape(TOKENS, TOP, D).sum(axis=1).astype(jnp.bfloat16)
    route_grad = expert_gate[position].reshape(TOKENS, TOP)
    return (tokens_grad, route_grad, gate_grad, up_grad, down_grad)
```

```python
import jax
import jax.numpy as jnp
from jax import lax
from jax.experimental import pallas as pl
from jax.experimental.pallas import tpu as pltpu
from jax.sharding import Mesh
from jax.sharding import PartitionSpec as P

EP = ("ep_0", "ep_1")
BF = jnp.bfloat16
F32 = jnp.float32

CAP = 18
SRC = 16
HALF_ROWS = SRC * CAP
PIECE = 40
BACK = 24
GATH = 2 * HALF_ROWS + 8
PART = HALF_ROWS + 8


def iota(shape, dim):
    return lax.broadcasted_iota(jnp.int32, shape, dim)


def one_if(cond):
    return jnp.where(cond, 1.0, 0.0).astype(BF)


def split_two(value):
    high = value.astype(BF)
    low = (value - high.astype(F32)).astype(BF)
    return high, low


def contract_cols(left, right):
    return lax.dot_general(left, right, (((1,), (1,)), ((), ())), preferred_element_type=F32)


def matmul(left, right):
    return lax.dot_general(left, right, (((1,), (0,)), ((), ())), preferred_element_type=F32)


def ranks(routes):
    count = routes.shape[0]
    lane = iota((count, 128), 1)
    first = routes[:, 0:1] == lane
    second = routes[:, 1:2] == lane
    member = jnp.where(first | second, 1.0, 0.0)
    before = one_if(iota((count, count), 1) < iota((count, count), 0))
    rank = matmul(before, member.astype(BF))
    return first, second, member, rank


def dispatch_kernel(where_ref, routes_ref, weights_ref, tokens_ref, grad_ref, out_ref):
    first, second, member, rank = ranks(routes_ref[...])
    weights = weights_ref[...]
    weight = jnp.where(first, weights[:, 0:1], 0.0) + jnp.where(second, weights[:, 1:2], 0.0)
    slot = jnp.where(member > 0.0, rank, -100.0)
    slot_t = jnp.transpose(slot)[:16]
    weight_t = jnp.transpose(weight)[:16]
    row = iota((16, PIECE, 128), 1)
    slot_3 = jnp.broadcast_to(slot_t.astype(jnp.int32)[:, None, :], (16, PIECE, 128))
    sel_x = jnp.where(slot_3 == row, 1.0, 0.0)
    sel_dy = jnp.where(slot_3 + CAP == row, 1.0, 0.0)
    chosen = jnp.concatenate(
        [sel_x.reshape(16 * PIECE, 128).astype(BF), sel_dy.reshape(16 * PIECE, 128).astype(BF)], axis=1
    )
    rows = matmul(chosen, jnp.concatenate([tokens_ref[...], grad_ref[...]], axis=0))
    value = jnp.sum(sel_x * weight_t[:, None, :], axis=2, keepdims=True)
    offset = (where_ref[1] % 4) * 32
    spread = jnp.where(iota((16, PIECE, 128), 2) == row + offset, value, 0.0)
    packed = jnp.sum(jnp.where(row < CAP, spread, 0.0), axis=1, keepdims=True)
    high = packed.astype(BF).astype(F32)
    low = packed - high
    rows = rows.reshape(16, PIECE, 128)
    rows = jnp.where(row == 36, high, jnp.where(row == 37, low, rows))
    out_ref[...] = rows.reshape(16 * PIECE, 128).astype(BF)


def copies_kernel(in_ref, out_ref):
    p = iota((2 * HALF_ROWS, 1), 0)
    is_dy = p >= HALF_ROWS
    q = jnp.where(is_dy, p - HALF_ROWS, p)
    source = (q * 3641) >> 16
    target = source * PIECE + (q - source * CAP) + jnp.where(is_dy, CAP, 0)
    pick = one_if(iota((2 * HALF_ROWS, SRC * PIECE), 1) == target)
    col = iota((8, SRC * PIECE), 1)
    of_source = (col * 1639) >> 16
    within = col - of_source * PIECE
    i = iota((8, SRC * PIECE), 0)
    is_low = i >= 4
    group = jnp.where(is_low, i - 4, i)
    pick_w = one_if(((of_source >> 2) == group) & (within == jnp.where(is_low, 37, 36)))
    data = in_ref[...]
    rows = matmul(pick, data).astype(BF)
    extra = matmul(pick_w, data).astype(BF)
    for t in range(16):
        out_ref[t, 0 : 2 * HALF_ROWS, :] = rows
        out_ref[t, 2 * HALF_ROWS : GATH, :] = extra


def lane_of_row():
    r = iota((HALF_ROWS, 1), 0)
    source = (r * 3641) >> 16
    lane = (source & 3) * 32 + (r - source * CAP)
    return source >> 2, lane


def row_weights(extra):
    group, lane = lane_of_row()
    spread = matmul(one_if((iota((HALF_ROWS, 8), 1) & 3) == group), extra)
    return jnp.sum(jnp.where(iota((HALF_ROWS, 128), 1) == lane, spread, 0.0), axis=1, keepdims=True)


def pair_cols(ref, t, start):
    return jnp.concatenate(
        [ref[2 * t, start : start + HALF_ROWS, :], ref[2 * t + 1, start : start + HALF_ROWS, :]], axis=1
    )


def main_kernel(
    own_ref, other_ref, gate_ref, up_ref, down_ref, part_own_ref, part_other_ref, both_ref, hidden_ref
):
    for k, (ref, out_ref) in enumerate(((own_ref, part_own_ref), (other_ref, part_other_ref))):
        pre = jnp.zeros((HALF_ROWS, 256), F32)
        d_hidden = jnp.zeros((HALF_ROWS, 128), F32)
        for t in range(8):
            cols = slice(256 * t, 256 * t + 256)
            proj = jnp.concatenate([gate_ref[cols, :], up_ref[cols, :]], axis=1)
            pre = pre + matmul(pair_cols(ref, t, 0), proj)
            d_hidden = d_hidden + contract_cols(pair_cols(ref, t, HALF_ROWS), down_ref[:, cols])
        pre_gate = pre[:, :128]
        pre_up = pre[:, 128:]
        sigma = jax.nn.sigmoid(pre_gate)
        activ = pre_gate * sigma
        hidden = activ * pre_up
        gate_part = jnp.sum(hidden * d_hidden, axis=1, keepdims=True)
        g = row_weights(ref[0, 2 * HALF_ROWS : GATH, :])
        scaled = g * d_hidden
        d_gate = scaled * pre_up * sigma * (1.0 + pre_gate * (1.0 - sigma))
        d_up = scaled * activ
        both = jnp.concatenate([d_gate.astype(BF), d_up.astype(BF)], axis=1)
        both_ref[k * HALF_ROWS : (k + 1) * HALF_ROWS, :] = both
        hidden_ref[k * HALF_ROWS : (k + 1) * HALF_ROWS, :] = hidden.astype(BF)
        _, lane = lane_of_row()
        spread = jnp.where(iota((HALF_ROWS, 128), 1) == lane, gate_part, 0.0)
        packed = jnp.sum(spread.reshape(4, HALF_ROWS // 4, 128), axis=1)
        extra = jnp.concatenate(split_two(packed), axis=0)
        for t in range(8):
            cols = slice(256 * t, 256 * t + 256)
            proj = jnp.concatenate([gate_ref[cols, :], up_ref[cols, :]], axis=1)
            value = contract_cols(both, proj).astype(BF)
            out_ref[2 * t, 0:HALF_ROWS, :] = value[:, :128]
            out_ref[2 * t + 1, 0:HALF_ROWS, :] = value[:, 128:]
            out_ref[2 * t, HALF_ROWS:PART, :] = extra
            out_ref[2 * t + 1, HALF_ROWS:PART, :] = extra


def weights_kernel(own_ref, other_ref, both_ref, hidden_ref, gate_out, up_out, down_out):
    both_t = jnp.transpose(both_ref[...].astype(F32)).astype(BF)
    hidden_t = jnp.transpose(hidden_ref[...].astype(F32)).astype(BF)
    g_own = row_weights(own_ref[0, 2 * HALF_ROWS : GATH, :])
    g_other = row_weights(other_ref[0, 2 * HALF_ROWS : GATH, :])
    for t in range(8):
        cols = slice(256 * t, 256 * t + 256)
        x = jnp.concatenate([pair_cols(own_ref, t, 0), pair_cols(other_ref, t, 0)], axis=0)
        grads = jnp.transpose(matmul(both_t, x))
        gate_out[cols, :] = grads[:, :128].astype(BF)
        up_out[cols, :] = grads[:, 128:].astype(BF)
        scaled = jnp.concatenate(
            [
                (g_own * pair_cols(own_ref, t, HALF_ROWS).astype(F32)).astype(BF),
                (g_other * pair_cols(other_ref, t, HALF_ROWS).astype(F32)).astype(BF),
            ],
            axis=0,
        )
        down_out[:, cols] = matmul(hidden_t, scaled).astype(BF)


def add_kernel(own_ref, other_ref, out_ref):
    def packed(ref):
        extra = ref[0, HALF_ROWS:PART, :].astype(F32)
        return extra[0:4] + extra[4:8]

    extra = jnp.concatenate(split_two(packed(own_ref) + packed(other_ref)), axis=0)
    for t in range(16):
        rows = own_ref[t, 0:HALF_ROWS, :].astype(F32) + other_ref[t, 0:HALF_ROWS, :].astype(F32)
        out_ref[t, 0:HALF_ROWS, :] = rows.astype(BF)
        out_ref[t, HALF_ROWS:PART, :] = extra


def sum_kernel(in_ref, out_ref):
    rows = in_ref[0, 0:HALF_ROWS, :].astype(F32)
    extra = in_ref[0, HALF_ROWS:PART, :].astype(F32)
    for t in range(1, 16):
        rows = rows + in_ref[t, 0:HALF_ROWS, :].astype(F32)
        extra = extra + in_ref[t, HALF_ROWS:PART, :].astype(F32)
    p = iota((SRC * BACK, 1), 0)
    source = (p * 2731) >> 16
    j = p - source * BACK
    target = jnp.where(j < CAP, source * CAP + j, -1)
    pick = one_if(iota((SRC * BACK, HALF_ROWS), 1) == target)
    col = iota((SRC * BACK, 8), 1)
    group = source >> 2
    pick_g = one_if(((j == 18) & (col == group)) | ((j == 19) & (col == group + 4)))
    packed = jnp.concatenate(split_two(extra[0:4] + extra[4:8]), axis=0)
    out_ref[...] = (matmul(pick, rows.astype(BF)) + matmul(pick_g, packed)).astype(BF)


def combine_kernel(where_ref, routes_ref, in_ref, tokens_ref, route_ref):
    routes = routes_ref[...]
    count = routes.shape[0]
    first, second, member, rank = ranks(routes)
    slot = jnp.where(member > 0.0, rank, -1.0).astype(BF)
    p = iota((1, 16 * BACK), 1)
    expert = (p * 2731) >> 16
    j = p - expert * BACK
    spread = matmul(slot, one_if(iota((128, 16 * BACK), 0) == expert))
    data = in_ref[...]
    tokens_ref[...] = matmul(one_if(spread.astype(jnp.int32) == j), data).astype(BF)
    offset = (where_ref[1] % 4) * 32
    lane = iota((count, 128), 1)
    is_gate = (j == 18) | (j == 19)
    for k, mine in enumerate((first, second)):
        values = matmul(one_if((routes[:, k : k + 1] == expert) & is_gate), data)
        index = jnp.sum(jnp.where(mine, rank, 0.0), axis=1, keepdims=True).astype(jnp.int32)
        route_ref[:, k : k + 1] = jnp.sum(
            jnp.where(lane == index + offset, values, 0.0), axis=1, keepdims=True
        )


def shape(dims, dtype=BF):
    return jax.ShapeDtypeStruct(dims, dtype)


def whole(dims):
    return pl.BlockSpec(dims, lambda i, *_: (0,) * len(dims))


def local(tokens, routes, route_weights, out_grad, gate_proj, up_proj, down_proj):
    count, width = tokens.shape
    where = jnp.stack([lax.axis_index("tp"), lax.axis_index("ep_0")]).astype(jnp.int32)
    columns = pl.BlockSpec((count, 128), lambda i, w: (0, w[0]))
    pieces = pl.pallas_call(
        dispatch_kernel,
        grid_spec=pltpu.PrefetchScalarGridSpec(
            num_scalar_prefetch=1,
            grid=(1,),
            in_specs=[whole(routes.shape), whole(route_weights.shape), columns, columns],
            out_specs=whole((16 * PIECE, 128)),
        ),
        out_shape=shape((16 * PIECE, 128)),
        name="dispatch",
    )(where, routes, route_weights, tokens, out_grad)
    received = lax.all_to_all(pieces.reshape(16, PIECE, 128), "ep_0", 0, 0, tiled=True)
    copies = pl.pallas_call(copies_kernel, out_shape=shape((16, GATH, 128)), name="copies")(
        received.reshape(SRC * PIECE, 128)
    )
    own = lax.all_to_all(copies, "tp", 0, 0, tiled=True)
    swap = [(0, 1), (1, 0)]
    other = lax.ppermute(own, "ep_1", swap)
    gate, up, down = gate_proj[0], up_proj[0], down_proj[0]
    part_own, part_other, both, hidden = pl.pallas_call(
        main_kernel,
        out_shape=(
            shape((16, PART, 128)),
            shape((16, PART, 128)),
            shape((2 * HALF_ROWS, 256)),
            shape((2 * HALF_ROWS, 128)),
        ),
        name="main",
    )(own, other, gate, up, down)
    part_received = lax.ppermute(part_other, "ep_1", swap)
    summed = pl.pallas_call(add_kernel, out_shape=shape((16, PART, 128)), name="add")(
        part_own, part_received
    )
    spread = lax.all_to_all(summed, "tp", 0, 0, tiled=True)
    gate_grad, up_grad, down_grad = pl.pallas_call(
        weights_kernel,
        out_shape=(shape((width, 128)), shape((width, 128)), shape((128, width))),
        name="weights",
    )(own, other, both, hidden)
    back = pl.pallas_call(sum_kernel, out_shape=shape((SRC * BACK, 128)), name="sum")(spread)
    home = lax.all_to_all(back.reshape(SRC, BACK, 128), "ep_0", 0, 0, tiled=True)
    tokens_grad, route_grad = pl.pallas_call(
        combine_kernel,
        grid_spec=pltpu.PrefetchScalarGridSpec(
            num_scalar_prefetch=1,
            grid=(1,),
            in_specs=[whole(routes.shape), whole((16 * BACK, 128))],
            out_specs=(whole((count, 128)), whole(routes.shape)),
        ),
        out_shape=(shape((count, 128)), shape(routes.shape, F32)),
        name="combine",
    )(where, routes, home.reshape(16 * BACK, 128))
    return (tokens_grad, route_grad, gate_grad[None], up_grad[None], down_grad[None])


def solution(mesh):
    torus = Mesh(mesh.devices.reshape(16, 2, mesh.shape["tp"]), ("ep_0", "ep_1", "tp"))
    placed = (
        P(EP, None),
        P(EP, None),
        P(EP, None),
        P(EP, None),
        P(EP, None, "tp"),
        P(EP, None, "tp"),
        P(EP, "tp", None),
    )
    return jax.shard_map(
        local,
        mesh=torus,
        in_specs=placed,
        out_specs=(
            P(EP, "tp"),
            P(EP, None),
            P(EP, None, "tp"),
            P(EP, None, "tp"),
            P(EP, "tp", None),
        ),
        check_vma=False,
    )
```

```python
import jax
import jax.numpy as jnp
from jax import lax
from jax.experimental import pallas as pl
from jax.experimental.pallas import tpu as pltpu
from jax.sharding import Mesh
from jax.sharding import PartitionSpec as P


EP = ("ep_0", "ep_1")
BF = jnp.bfloat16
F32 = jnp.float32

CAP = 18
SRC = 16
ROWS = SRC * CAP
PIECE = 40
BACK = 24
GATH = 2 * ROWS + 8
LIMIT = pltpu.CompilerParams(vmem_limit_bytes=24 * 1024 * 1024)
PART = ROWS + 8


def iota(shape, dim):
    return lax.broadcasted_iota(jnp.int32, shape, dim)


def one_if(cond):
    return jnp.where(cond, 1.0, 0.0).astype(BF)


def split_two(value):
    high = value.astype(BF)
    low = (value - high.astype(F32)).astype(BF)
    return high, low


def contract_cols(left, right):
    return lax.dot_general(left, right, (((1,), (1,)), ((), ())), preferred_element_type=F32)


def matmul(left, right):
    return lax.dot_general(left, right, (((1,), (0,)), ((), ())), preferred_element_type=F32)


def ranks(routes):
    count = routes.shape[1]
    expert = iota((16, count), 0)
    first = routes[0:1, :] == expert
    second = routes[1:2, :] == expert
    member = jnp.where(first | second, 1.0, 0.0)
    before = one_if(iota((count, count), 0) < iota((count, count), 1))
    rank = matmul(member.astype(BF), before)
    return first, second, member, rank


def dispatch_kernel(routes_ref, weights_ref, tokens_ref, grad_ref, out_ref, data_ref, sems):
    start = pl.multiple_of(lax.axis_index("tp") * 128, 128)
    loads = [
        pltpu.make_async_copy(
            ref.at[:, pl.ds(start, 128)], data_ref.at[pl.ds(128 * k, 128), :], sems.at[k]
        )
        for k, ref in enumerate((tokens_ref, grad_ref))
    ]
    for load in loads:
        load.start()
    first, second, member, rank = ranks(routes_ref[...])
    weights = weights_ref[...]
    weight = jnp.where(first, weights[0:1, :], 0.0) + jnp.where(second, weights[1:2, :], 0.0)
    slot = jnp.where(member > 0.0, rank, -100.0).astype(jnp.int32)
    row = iota((16, PIECE, 128), 1)
    slot_3 = jnp.broadcast_to(slot[:, None, :], (16, PIECE, 128))
    sel_x = jnp.where(slot_3 == row, 1.0, 0.0)
    sel_dy = jnp.where(slot_3 + CAP == row, 1.0, 0.0)
    chosen = jnp.concatenate(
        [sel_x.reshape(16 * PIECE, 128).astype(BF), sel_dy.reshape(16 * PIECE, 128).astype(BF)], axis=1
    )
    value = jnp.sum(sel_x * weight[:, None, :], axis=2, keepdims=True)
    offset = (lax.axis_index("ep_0") % 4) * 32
    spread = jnp.where(iota((16, PIECE, 128), 2) == row + offset, value, 0.0)
    packed = jnp.sum(jnp.where(row < CAP, spread, 0.0), axis=1, keepdims=True)
    high = packed.astype(BF).astype(F32)
    low = packed - high
    for load in loads:
        load.wait()
    rows = matmul(chosen, data_ref[...]).reshape(16, PIECE, 128)
    rows = jnp.where(row == 36, high, jnp.where(row == 37, low, rows))
    out_ref[...] = rows.reshape(16 * PIECE, 128).astype(BF)


def plan_kernel(routes_ref, copies_ref, back_ref, combine_ref, lanes_ref):
    p = iota((2 * ROWS, 1), 0)
    is_dy = p >= ROWS
    q = jnp.where(is_dy, p - ROWS, p)
    source = (q * 3641) >> 16
    target = source * PIECE + (q - source * CAP) + jnp.where(is_dy, CAP, 0)
    copies_ref[0 : 2 * ROWS, :] = one_if(iota((2 * ROWS, SRC * PIECE), 1) == target)
    col = iota((16, SRC * PIECE), 1)
    of_source = (col * 1639) >> 16
    within = col - of_source * PIECE
    i = iota((16, SRC * PIECE), 0)
    pick = ((of_source >> 2) == (i & 3)) & (within == jnp.where(i >= 4, 37, 36)) & (i < 8)
    copies_ref[2 * ROWS : 2 * ROWS + 16, :] = one_if(pick)

    p = iota((SRC * BACK, 1), 0)
    source = (p * 2731) >> 16
    j = p - source * BACK
    target = jnp.where(j < CAP, source * CAP + j, -1)
    target = jnp.where(j == 18, ROWS + (source >> 2), target)
    target = jnp.where(j == 19, ROWS + 4 + (source >> 2), target)
    back_ref[...] = one_if(iota((SRC * BACK, PART), 1) == target)

    routes = routes_ref[...]
    first, second, member, rank = ranks(routes)
    slot = jnp.where(member > 0.0, rank, -100.0).astype(jnp.int32)
    row = iota((16, BACK, 128), 1)
    sel = jnp.where(jnp.broadcast_to(slot[:, None, :], (16, BACK, 128)) == row, 1.0, 0.0)
    combine_ref[0:128, :] = jnp.transpose(sel.reshape(16 * BACK, 128)).astype(BF)
    offset = (lax.axis_index("ep_0") % 4) * 32
    is_gate = (row == 18) | (row == 19)
    for k, mine in enumerate((first, second)):
        chosen = jnp.where(mine, 1.0, 0.0)[:, None, :]
        sel = jnp.where(is_gate, jnp.broadcast_to(chosen, (16, BACK, 128)), 0.0)
        combine_ref[128 * (k + 1) : 128 * (k + 2), :] = jnp.transpose(
            sel.reshape(16 * BACK, 128)
        ).astype(BF)
        index = jnp.sum(jnp.where(mine, rank, 0.0), axis=0, keepdims=True).astype(jnp.int32)
        lanes = jnp.where(iota((128, 128), 0) == index + offset, 1.0, 0.0)
        lanes_ref[128 * k : 128 * (k + 1), :] = jnp.transpose(lanes).astype(BF)


def copies_kernel(in_ref, pick_ref, out_ref):
    rows = matmul(pick_ref[...], in_ref[...]).astype(BF)
    for t in range(16):
        out_ref[t] = rows[:GATH]


def lane_of_row():
    r = iota((ROWS, 1), 0)
    source = (r * 3641) >> 16
    lane = (source & 3) * 32 + (r - source * CAP)
    return source >> 2, lane


def row_weights(extra):
    group, lane = lane_of_row()
    spread = matmul(one_if((iota((ROWS, 8), 1) & 3) == group), extra)
    return jnp.sum(jnp.where(iota((ROWS, 128), 1) == lane, spread, 0.0), axis=1, keepdims=True)


def pair_cols(ref, t, start):
    return jnp.concatenate([ref[2 * t, start : start + ROWS, :], ref[2 * t + 1, start : start + ROWS, :]], axis=1)


def main_kernel(own_ref, *refs):
    weights, (part_out, both_ref, hidden_ref) = refs[:6], refs[6:9]
    held, (part_ref, both_held, hidden_held), (in_sems, out_sems) = refs[9:15], refs[15:18], refs[18:20]
    loads = []
    for s in range(4):
        stage = []
        for k in range(6):
            part = pl.ds(512 * s, 512)
            index = (slice(None), part) if k % 3 == 2 else (part, slice(None))
            stage.append(
                pltpu.make_async_copy(weights[k].at[index], held[k].at[index], in_sems.at[6 * s + k])
            )
            stage[-1].start()
        loads.append(stage)
    gate, up, down, gate_2, up_2, down_2 = held
    pre_gate = jnp.zeros((ROWS, 256), F32)
    pre_up = jnp.zeros((ROWS, 256), F32)
    d_hidden = jnp.zeros((ROWS, 256), F32)
    for t in range(8):
        if t % 2 == 0:
            for load in loads[t // 2]:
                load.wait()
        cols = slice(256 * t, 256 * t + 256)
        x = pair_cols(own_ref, t, 0)
        pre_gate = pre_gate + matmul(x, jnp.concatenate([gate[cols, :], gate_2[cols, :]], axis=1))
        pre_up = pre_up + matmul(x, jnp.concatenate([up[cols, :], up_2[cols, :]], axis=1))
        d_hidden = d_hidden + contract_cols(
            pair_cols(own_ref, t, ROWS), jnp.concatenate([down[:, cols], down_2[:, cols]], axis=0)
        )
    sigma = jax.nn.sigmoid(pre_gate)
    activ = pre_gate * sigma
    hidden = activ * pre_up
    gate_part = jnp.sum(hidden * d_hidden, axis=1, keepdims=True)
    scaled = row_weights(own_ref[0, 2 * ROWS : GATH, :]) * d_hidden
    d_gate = (scaled * pre_up * sigma * (1.0 + pre_gate * (1.0 - sigma))).astype(BF)
    d_up = (scaled * activ).astype(BF)
    both_held[:, 0:256] = d_gate
    both_held[:, 256:512] = d_up
    hidden_held[...] = hidden.astype(BF)
    stores = [
        pltpu.make_async_copy(both_held, both_ref, out_sems.at[0]),
        pltpu.make_async_copy(hidden_held, hidden_ref, out_sems.at[1]),
    ]
    for store in stores:
        store.start()
    _, lane = lane_of_row()
    spread = jnp.where(iota((ROWS, 128), 1) == lane, gate_part, 0.0)
    packed = jnp.sum(spread.reshape(4, ROWS // 4, 128), axis=1)
    extra = jnp.concatenate(split_two(packed), axis=0)
    for t in range(8):
        cols = slice(256 * t, 256 * t + 256)
        value = contract_cols(d_gate, jnp.concatenate([gate[cols, :], gate_2[cols, :]], axis=1))
        value = value + contract_cols(d_up, jnp.concatenate([up[cols, :], up_2[cols, :]], axis=1))
        value = value.astype(BF)
        for k in range(2):
            part_ref[2 * t + k, 0:ROWS, :] = value[:, 128 * k : 128 * k + 128]
            part_ref[2 * t + k, ROWS:PART, :] = extra
        two = pl.ds(2 * t, 2)
        stores.append(pltpu.make_async_copy(part_ref.at[two], part_out.at[two], out_sems.at[2 + t]))
        stores[-1].start()
    for store in stores:
        store.wait()


def half_grads(own_ref, both_ref, hidden_ref, half):
    lanes = slice(128 * half, 128 * half + 128)
    late = slice(256 + 128 * half, 256 + 128 * half + 128)
    both = jnp.concatenate([both_ref[:, lanes], both_ref[:, late]], axis=1)
    both_t = jnp.transpose(both.astype(F32)).astype(BF)
    hidden_t = jnp.transpose(hidden_ref[:, lanes].astype(F32)).astype(BF)
    g = row_weights(own_ref[0, 2 * ROWS : GATH, :])
    for t in range(8):
        cols = slice(256 * t, 256 * t + 256)
        scaled = (g * pair_cols(own_ref, t, ROWS).astype(F32)).astype(BF)
        yield cols, matmul(both_t, pair_cols(own_ref, t, 0)), matmul(hidden_t, scaled)


def partner_grads_kernel(own_ref, both_ref, hidden_ref, out_ref):
    for cols, both, down in half_grads(own_ref, both_ref, hidden_ref, 1):
        out_ref[0:256, cols] = both.astype(BF)
        out_ref[256:384, cols] = down.astype(BF)


def own_grads_kernel(own_ref, both_ref, hidden_ref, other_ref, gate_out, up_out, down_out):
    for cols, both, down in half_grads(own_ref, both_ref, hidden_ref, 0):
        grads = jnp.transpose(both + other_ref[0:256, cols].astype(F32))
        gate_out[cols, :] = grads[:, :128].astype(BF)
        up_out[cols, :] = grads[:, 128:].astype(BF)
        down_out[:, cols] = (down + other_ref[256:384, cols].astype(F32)).astype(BF)


def sum_kernel(in_ref, pick_ref, out_ref):
    rows = in_ref[0].astype(F32)
    for t in range(1, 16):
        rows = rows + in_ref[t].astype(F32)
    packed = rows[ROWS : ROWS + 4] + rows[ROWS + 4 : PART]
    high = packed.astype(BF).astype(F32)
    rows = jnp.concatenate([rows[:ROWS], high, packed - high], axis=0).astype(BF)
    out_ref[...] = matmul(pick_ref[...], rows).astype(BF)


def combine_kernel(in_ref, pick_ref, lanes_ref, tokens_ref, route_ref):
    values = matmul(pick_ref[...], in_ref[...])
    tokens_ref[...] = values[:128].astype(BF)
    gates = lax.dot_general(
        jnp.ones((8, 128), F32),
        values[128:] * lanes_ref[...].astype(F32),
        (((1,), (1,)), ((), ())),
        precision=lax.Precision.HIGHEST,
        preferred_element_type=F32,
    )
    route_ref[0:1, :] = gates[0:1, :128]
    route_ref[1:2, :] = gates[0:1, 128:]


def shape(dims, dtype=BF):
    return jax.ShapeDtypeStruct(dims, dtype)


def far_shape(dims, dtype=BF):
    return pltpu.HBM(dims, dtype)


def near(dims, dtype=BF):
    return pltpu.VMEM(dims, dtype)


def far(value):
    return pltpu.with_memory_space_constraint(value, pltpu.HBM)


def hold(value):
    return pltpu.with_memory_space_constraint(value, pltpu.VMEM)


def local(tokens, routes, route_weights, out_grad, gate_proj, up_proj, down_proj):
    return steps(tokens, routes, route_weights, out_grad, gate_proj[0], up_proj[0], down_proj[0])


def exchange(value, axis):
    return lax.all_to_all(value, axis, 0, 0, tiled=True)


def to_partner(value):
    return lax.ppermute(value, "ep_1", [(0, 1), (1, 0)])


def kernel(body, **settings):
    return pl.pallas_call(body, compiler_params=LIMIT, **settings)


def steps(tokens, routes, route_weights, out_grad, gate, up, down):
    count, width = tokens.shape
    routes_t = routes.T
    weights_t = route_weights.T
    vmem = pl.BlockSpec(memory_space=pltpu.VMEM)
    hbm = pl.BlockSpec(memory_space=pltpu.HBM)
    pieces = kernel(
        dispatch_kernel,
        in_specs=[vmem, vmem, hbm, hbm],
        out_shape=near((16 * PIECE, 128)),
        scratch_shapes=[pltpu.VMEM((256, 128), BF), pltpu.SemaphoreType.DMA((2,))],
    )(routes_t, weights_t, far(tokens), far(out_grad))
    received = exchange(pieces.reshape(16, PIECE, 128), "ep_0")
    gate_2, up_2, down_2 = (to_partner(w) for w in (gate, up, down))
    pick_copies, pick_back, pick_combine, lanes = kernel(
        plan_kernel,
        out_shape=(
            near((2 * ROWS + 16, SRC * PIECE)),
            shape((SRC * BACK, PART)),
            shape((384, 16 * BACK)),
            shape((256, 128)),
        ),
    )(routes_t)
    received, gate_2, up_2, down_2 = lax.optimization_barrier((received, gate_2, up_2, down_2))
    copies = kernel(copies_kernel, out_shape=near((16, GATH, 128)))(
        hold(received.reshape(SRC * PIECE, 128)), hold(pick_copies)
    )
    own = exchange(copies, "tp")
    part, both, hidden = kernel(
        main_kernel,
        in_specs=[vmem] + [hbm] * 6,
        out_specs=(hbm, hbm, hbm),
        out_shape=(far_shape((16, PART, 128)), far_shape((ROWS, 512)), far_shape((ROWS, 256))),
        scratch_shapes=[
            *[pltpu.VMEM(w.shape, BF) for w in (gate, up, down, gate, up, down)],
            pltpu.VMEM((16, PART, 128), BF),
            pltpu.VMEM((ROWS, 512), BF),
            pltpu.VMEM((ROWS, 256), BF),
            pltpu.SemaphoreType.DMA((24,)),
            pltpu.SemaphoreType.DMA((10,)),
        ],
    )(hold(own), *(far(w) for w in (gate, up, down, gate_2, up_2, down_2)))
    spread = exchange(part, "tp")
    partner = kernel(partner_grads_kernel, out_shape=shape((384, width)))(own, both, hidden)
    mine = to_partner(partner)
    gate_grad, up_grad, down_grad = kernel(
        own_grads_kernel, out_shape=(shape((width, 128)), shape((width, 128)), shape((128, width)))
    )(own, both, hidden, mine)
    back = kernel(sum_kernel, out_shape=near((SRC * BACK, 128)))(hold(spread), hold(pick_back))
    home = exchange(back.reshape(SRC, BACK, 128), "ep_0")
    tokens_grad, route_grad = kernel(
        combine_kernel, out_shape=(shape((count, 128)), shape((2, count), F32))
    )(hold(home.reshape(16 * BACK, 128)), hold(pick_combine), hold(lanes))
    return (tokens_grad, route_grad.T, gate_grad[None], up_grad[None], down_grad[None])


def solution(mesh):
    torus = Mesh(mesh.devices.reshape(16, 2, mesh.shape["tp"]), ("ep_0", "ep_1", "tp"))
    placed = (
        P(EP, None),
        P(EP, None),
        P(EP, None),
        P(EP, None),
        P(EP, None, "tp"),
        P(EP, None, "tp"),
        P(EP, "tp", None),
    )
    return jax.shard_map(
        local,
        mesh=torus,
        in_specs=placed,
        out_specs=(
            P(EP, "tp"),
            P(EP, None),
            P(EP, None, "tp"),
            P(EP, None, "tp"),
            P(EP, "tp", None),
        ),
        check_vma=False,
    )
```

```python
import jax
import jax.numpy as jnp
from jax import lax
from jax.experimental import pallas as pl
from jax.experimental.pallas import tpu as pltpu
from jax.sharding import Mesh
from jax.sharding import PartitionSpec as P


EP = ("ep_0", "ep_1")
BF = jnp.bfloat16
F32 = jnp.float32

CAP = 18
SRC = 16
ROWS = SRC * CAP
PIECE = 40
BACK = 24
GATH = 2 * ROWS + 8
LIMIT = pltpu.CompilerParams(vmem_limit_bytes=24 * 1024 * 1024)
PART = ROWS + 8


def iota(shape, dim):
    return lax.broadcasted_iota(jnp.int32, shape, dim)


def one_if(cond):
    return jnp.where(cond, 1.0, 0.0).astype(BF)


def split_two(value):
    high = value.astype(BF)
    low = (value - high.astype(F32)).astype(BF)
    return high, low


def contract_cols(left, right):
    return lax.dot_general(left, right, (((1,), (1,)), ((), ())), preferred_element_type=F32)


def matmul(left, right):
    return lax.dot_general(left, right, (((1,), (0,)), ((), ())), preferred_element_type=F32)


def ranks(routes):
    count = routes.shape[1]
    expert = iota((16, count), 0)
    first = routes[0:1, :] == expert
    second = routes[1:2, :] == expert
    member = jnp.where(first | second, 1.0, 0.0)
    before = one_if(iota((count, count), 0) < iota((count, count), 1))
    rank = matmul(member.astype(BF), before)
    return first, second, member, rank


def dispatch_kernel(
    routes_hbm, weights_hbm, tokens_ref, grad_ref, out_ref, data_ref, routes_ref, weights_ref, sems
):
    start = pl.multiple_of(lax.axis_index("tp") * 128, 128)
    small = [
        pltpu.make_async_copy(routes_hbm, routes_ref, sems.at[2]),
        pltpu.make_async_copy(weights_hbm, weights_ref, sems.at[3]),
    ]
    loads = [
        pltpu.make_async_copy(
            ref.at[:, pl.ds(start, 128)], data_ref.at[pl.ds(128 * k, 128), :], sems.at[k]
        )
        for k, ref in enumerate((tokens_ref, grad_ref))
    ]
    for load in small + loads:
        load.start()
    for load in small:
        load.wait()
    first, second, member, rank = ranks(routes_ref[...])
    weights = weights_ref[...]
    weight = jnp.where(first, weights[0:1, :], 0.0) + jnp.where(second, weights[1:2, :], 0.0)
    slot = jnp.where(member > 0.0, rank, -100.0).astype(jnp.int32)
    row = iota((16, PIECE, 128), 1)
    slot_3 = jnp.broadcast_to(slot[:, None, :], (16, PIECE, 128))
    sel_x = jnp.where(slot_3 == row, 1.0, 0.0)
    sel_dy = jnp.where(slot_3 + CAP == row, 1.0, 0.0)
    chosen = jnp.concatenate(
        [sel_x.reshape(16 * PIECE, 128).astype(BF), sel_dy.reshape(16 * PIECE, 128).astype(BF)], axis=1
    )
    value = jnp.sum(sel_x * weight[:, None, :], axis=2, keepdims=True)
    offset = (lax.axis_index("ep_0") % 4) * 32
    spread = jnp.where(iota((16, PIECE, 128), 2) == row + offset, value, 0.0)
    packed = jnp.sum(jnp.where(row < CAP, spread, 0.0), axis=1, keepdims=True)
    high = packed.astype(BF).astype(F32)
    low = packed - high
    for load in loads:
        load.wait()
    rows = matmul(chosen, data_ref[...]).reshape(16, PIECE, 128)
    rows = jnp.where(row == 36, high, jnp.where(row == 37, low, rows))
    out_ref[...] = rows.reshape(16 * PIECE, 128).astype(BF)


def plan_kernel(
    routes_hbm, gate, up, down, copies_ref, back_ref, combine_ref, lanes_ref, swap_ref, routes_ref, sems
):
    routes_load = pltpu.make_async_copy(routes_hbm, routes_ref, sems.at[18])
    routes_load.start()
    moves = [
        pltpu.make_async_copy(ref, swap_ref.at[pl.ds(2048 * k, 2048), :], sems.at[16 + k])
        for k, ref in enumerate((gate, up))
    ] + [
        pltpu.make_async_copy(
            down.at[:, pl.ds(128 * t, 128)], swap_ref.at[pl.ds(4096 + 128 * t, 128), :], sems.at[t]
        )
        for t in range(16)
    ]
    for move in moves:
        move.start()
    p = iota((2 * ROWS, 1), 0)
    is_dy = p >= ROWS
    q = jnp.where(is_dy, p - ROWS, p)
    source = (q * 3641) >> 16
    target = source * PIECE + (q - source * CAP) + jnp.where(is_dy, CAP, 0)
    copies_ref[0 : 2 * ROWS, :] = one_if(iota((2 * ROWS, SRC * PIECE), 1) == target)
    col = iota((16, SRC * PIECE), 1)
    of_source = (col * 1639) >> 16
    within = col - of_source * PIECE
    i = iota((16, SRC * PIECE), 0)
    pick = ((of_source >> 2) == (i & 3)) & (within == jnp.where(i >= 4, 37, 36)) & (i < 8)
    copies_ref[2 * ROWS : 2 * ROWS + 16, :] = one_if(pick)

    p = iota((SRC * BACK, 1), 0)
    source = (p * 2731) >> 16
    j = p - source * BACK
    target = jnp.where(j < CAP, source * CAP + j, -1)
    target = jnp.where(j == 18, ROWS + (source >> 2), target)
    target = jnp.where(j == 19, ROWS + 4 + (source >> 2), target)
    back_ref[...] = one_if(iota((SRC * BACK, PART), 1) == target)

    routes_load.wait()
    routes = routes_ref[...]
    first, second, member, rank = ranks(routes)
    slot = jnp.where(member > 0.0, rank, -100.0).astype(jnp.int32)
    row = iota((16, BACK, 128), 1)
    sel = jnp.where(jnp.broadcast_to(slot[:, None, :], (16, BACK, 128)) == row, 1.0, 0.0)
    combine_ref[0:128, :] = jnp.transpose(sel.reshape(16 * BACK, 128)).astype(BF)
    offset = (lax.axis_index("ep_0") % 4) * 32
    is_gate = (row == 18) | (row == 19)
    for k, mine in enumerate((first, second)):
        chosen = jnp.where(mine, 1.0, 0.0)[:, None, :]
        sel = jnp.where(is_gate, jnp.broadcast_to(chosen, (16, BACK, 128)), 0.0)
        combine_ref[128 * (k + 1) : 128 * (k + 2), :] = jnp.transpose(
            sel.reshape(16 * BACK, 128)
        ).astype(BF)
        index = jnp.sum(jnp.where(mine, rank, 0.0), axis=0, keepdims=True).astype(jnp.int32)
        lanes = jnp.where(iota((128, 128), 0) == index + offset, 1.0, 0.0)
        lanes_ref[128 * k : 128 * (k + 1), :] = jnp.transpose(lanes).astype(BF)
    for move in moves:
        move.wait()


def copies_kernel(in_ref, pick_ref, out_ref):
    rows = matmul(pick_ref[...], in_ref[...]).astype(BF)
    for t in range(16):
        out_ref[t] = rows[:GATH]


def lane_of_row():
    r = iota((ROWS, 1), 0)
    source = (r * 3641) >> 16
    lane = (source & 3) * 32 + (r - source * CAP)
    return source >> 2, lane


def row_weights(extra):
    group, lane = lane_of_row()
    spread = matmul(one_if((iota((ROWS, 8), 1) & 3) == group), extra)
    return jnp.sum(jnp.where(iota((ROWS, 128), 1) == lane, spread, 0.0), axis=1, keepdims=True)


def pair_cols(ref, t, start):
    return jnp.concatenate([ref[2 * t, start : start + ROWS, :], ref[2 * t + 1, start : start + ROWS, :]], axis=1)


def main_kernel(own_ref, gate, up, down, swap_ref, part_ref, both_ref, hidden_ref):
    pre_gate = jnp.zeros((ROWS, 256), F32)
    pre_up = jnp.zeros((ROWS, 256), F32)
    d_hidden = jnp.zeros((ROWS, 256), F32)

    def both_halves(ref, t, first):
        cols = slice(256 * t, 256 * t + 256)
        return jnp.concatenate([ref[cols, :], swap_ref[first + 256 * t : first + 256 * t + 256, :]], axis=1)

    for t in range(8):
        x = pair_cols(own_ref, t, 0)
        pre_gate = pre_gate + matmul(x, both_halves(gate, t, 0))
        pre_up = pre_up + matmul(x, both_halves(up, t, 2048))
        at = 4096 + 256 * t
        down_2 = jnp.concatenate([swap_ref[at : at + 128, :], swap_ref[at + 128 : at + 256, :]], axis=1)
        d_hidden = d_hidden + contract_cols(
            pair_cols(own_ref, t, ROWS),
            jnp.concatenate([down[:, 256 * t : 256 * t + 256], down_2], axis=0),
        )
    sigma = jax.nn.sigmoid(pre_gate)
    activ = pre_gate * sigma
    hidden = activ * pre_up
    gate_part = jnp.sum(hidden * d_hidden, axis=1, keepdims=True)
    scaled = row_weights(own_ref[0, 2 * ROWS : GATH, :]) * d_hidden
    d_gate = (scaled * pre_up * sigma * (1.0 + pre_gate * (1.0 - sigma))).astype(BF)
    d_up = (scaled * activ).astype(BF)
    both_ref[:, 0:256] = d_gate
    both_ref[:, 256:512] = d_up
    hidden_ref[...] = hidden.astype(BF)
    _, lane = lane_of_row()
    spread = jnp.where(iota((ROWS, 128), 1) == lane, gate_part, 0.0)
    packed = jnp.sum(spread.reshape(4, ROWS // 4, 128), axis=1)
    extra = jnp.concatenate(split_two(packed), axis=0)
    for t in range(8):
        value = contract_cols(d_gate, both_halves(gate, t, 0))
        value = value + contract_cols(d_up, both_halves(up, t, 2048))
        value = value.astype(BF)
        for k in range(2):
            part_ref[2 * t + k, 0:ROWS, :] = value[:, 128 * k : 128 * k + 128]
            part_ref[2 * t + k, ROWS:PART, :] = extra


def half_grads(own_ref, both_ref, hidden_ref, half):
    lanes = slice(128 * half, 128 * half + 128)
    late = slice(256 + 128 * half, 256 + 128 * half + 128)
    both = jnp.concatenate([both_ref[:, lanes], both_ref[:, late]], axis=1)
    both_t = jnp.transpose(both.astype(F32)).astype(BF)
    hidden_t = jnp.transpose(hidden_ref[:, lanes].astype(F32)).astype(BF)
    g = row_weights(own_ref[0, 2 * ROWS : GATH, :])
    for t in range(8):
        cols = slice(256 * t, 256 * t + 256)
        scaled = (g * pair_cols(own_ref, t, ROWS).astype(F32)).astype(BF)
        yield cols, matmul(both_t, pair_cols(own_ref, t, 0)), matmul(hidden_t, scaled)


def partner_grads_kernel(own_ref, both_ref, hidden_ref, out_ref):
    for cols, both, down in half_grads(own_ref, both_ref, hidden_ref, 1):
        out_ref[0:256, cols] = both.astype(BF)
        out_ref[256:384, cols] = down.astype(BF)


def own_grads_kernel(own_ref, both_ref, hidden_ref, other_ref, gate_out, up_out, down_out):
    for cols, both, down in half_grads(own_ref, both_ref, hidden_ref, 0):
        grads = jnp.transpose(both + other_ref[0:256, cols].astype(F32))
        gate_out[cols, :] = grads[:, :128].astype(BF)
        up_out[cols, :] = grads[:, 128:].astype(BF)
        down_out[:, cols] = (down + other_ref[256:384, cols].astype(F32)).astype(BF)


def sum_kernel(in_ref, pick_ref, out_ref):
    rows = in_ref[0].astype(F32)
    for t in range(1, 16):
        rows = rows + in_ref[t].astype(F32)
    packed = rows[ROWS : ROWS + 4] + rows[ROWS + 4 : PART]
    high = packed.astype(BF).astype(F32)
    rows = jnp.concatenate([rows[:ROWS], high, packed - high], axis=0).astype(BF)
    out_ref[...] = matmul(pick_ref[...], rows).astype(BF)


def combine_kernel(in_ref, pick_ref, lanes_ref, tokens_ref, route_ref):
    values = matmul(pick_ref[...], in_ref[...])
    tokens_ref[...] = values[:128].astype(BF)
    gates = lax.dot_general(
        jnp.ones((8, 128), F32),
        values[128:] * lanes_ref[...].astype(F32),
        (((1,), (1,)), ((), ())),
        precision=lax.Precision.HIGHEST,
        preferred_element_type=F32,
    )
    route_ref[0:1, :] = gates[0:1, :128]
    route_ref[1:2, :] = gates[0:1, 128:]


def shape(dims, dtype=BF):
    return jax.ShapeDtypeStruct(dims, dtype)


def far_shape(dims, dtype=BF):
    return pltpu.HBM(dims, dtype)


def near(dims, dtype=BF):
    return pltpu.VMEM(dims, dtype)


def far(value):
    return pltpu.with_memory_space_constraint(value, pltpu.HBM)


def hold(value):
    return pltpu.with_memory_space_constraint(value, pltpu.VMEM)


def local(tokens, routes, route_weights, out_grad, gate_proj, up_proj, down_proj):
    return steps(tokens, routes, route_weights, out_grad, gate_proj[0], up_proj[0], down_proj[0])


def exchange(value, axis):
    return lax.all_to_all(value, axis, 0, 0, tiled=True)


def to_partner(value):
    return lax.ppermute(value, "ep_1", [(0, 1), (1, 0)])


def kernel(body, **settings):
    return pl.pallas_call(body, compiler_params=LIMIT, **settings)


def steps(tokens, routes, route_weights, out_grad, gate, up, down):
    count, width = tokens.shape
    routes_t = routes.T
    weights_t = route_weights.T
    vmem = pl.BlockSpec(memory_space=pltpu.VMEM)
    hbm = pl.BlockSpec(memory_space=pltpu.HBM)
    small = [pltpu.VMEM((2, count), jnp.int32), pltpu.VMEM((2, count), F32)]
    pieces = kernel(
        dispatch_kernel,
        in_specs=[hbm] * 4,
        out_shape=near((16 * PIECE, 128)),
        scratch_shapes=[pltpu.VMEM((256, 128), BF), *small, pltpu.SemaphoreType.DMA((4,))],
    )(far(routes_t), far(weights_t), far(tokens), far(out_grad))
    received = exchange(pieces.reshape(16, PIECE, 128), "ep_0")
    pick_copies, pick_back, pick_combine, lanes, packed = kernel(
        plan_kernel,
        in_specs=[hbm] * 4,
        out_specs=(vmem, vmem, vmem, vmem, hbm),
        out_shape=(
            near((2 * ROWS + 16, SRC * PIECE)),
            shape((SRC * BACK, PART)),
            shape((384, 16 * BACK)),
            shape((256, 128)),
            far_shape((3 * width, 128)),
        ),
        scratch_shapes=[small[0], pltpu.SemaphoreType.DMA((19,))],
    )(far(routes_t), far(gate), far(up), far(down))
    packed_2 = to_partner(packed)
    received, packed_2 = lax.optimization_barrier((received, packed_2))
    copies = kernel(copies_kernel, out_shape=near((16, GATH, 128)))(
        hold(received.reshape(SRC * PIECE, 128)), hold(pick_copies)
    )
    own = hold(exchange(copies, "tp"))
    part, both, hidden = kernel(
        main_kernel,
        in_specs=[vmem] * 5,
        out_specs=(vmem, vmem, vmem),
        out_shape=(near((16, PART, 128)), near((ROWS, 512)), near((ROWS, 256))),
    )(own, gate, up, down, hold(packed_2))
    spread = exchange(part, "tp")
    partner = kernel(partner_grads_kernel, out_shape=shape((384, width)))(own, both, hidden)
    mine = to_partner(partner)
    gate_grad, up_grad, down_grad = kernel(
        own_grads_kernel, out_shape=(shape((width, 128)), shape((width, 128)), shape((128, width)))
    )(own, both, hidden, mine)
    back = kernel(sum_kernel, out_shape=near((SRC * BACK, 128)))(hold(spread), hold(pick_back))
    home = exchange(back.reshape(SRC, BACK, 128), "ep_0")
    tokens_grad, route_grad = kernel(
        combine_kernel, out_shape=(shape((count, 128)), shape((2, count), F32))
    )(hold(home.reshape(16 * BACK, 128)), hold(pick_combine), hold(lanes))
    return (tokens_grad, route_grad.T, gate_grad[None], up_grad[None], down_grad[None])


def solution(mesh):
    torus = Mesh(mesh.devices.reshape(16, 2, mesh.shape["tp"]), ("ep_0", "ep_1", "tp"))
    placed = (
        P(EP, None),
        P(EP, None),
        P(EP, None),
        P(EP, None),
        P(EP, None, "tp"),
        P(EP, None, "tp"),
        P(EP, "tp", None),
    )
    return jax.shard_map(
        local,
        mesh=torus,
        in_specs=placed,
        out_specs=(
            P(EP, "tp"),
            P(EP, None),
            P(EP, None, "tp"),
            P(EP, None, "tp"),
            P(EP, "tp", None),
        ),
        check_vma=False,
    )
```

```python
import jax
import jax.numpy as jnp
from jax import lax
from jax.experimental import pallas as pl
from jax.experimental.pallas import tpu as pltpu
from jax.sharding import Mesh
from jax.sharding import PartitionSpec as P


EP = ("ep_0", "ep_1")
BF = jnp.bfloat16
F32 = jnp.float32

CAP = 18
SRC = 16
ROWS = SRC * CAP
PIECE = 40
BACK = 24
GATH = 2 * ROWS + 8
LIMIT = pltpu.CompilerParams(vmem_limit_bytes=24 * 1024 * 1024)
PART = ROWS + 8


def iota(shape, dim):
    return lax.broadcasted_iota(jnp.int32, shape, dim)


def one_if(cond):
    return jnp.where(cond, 1.0, 0.0).astype(BF)


def split_two(value):
    high = value.astype(BF)
    low = (value - high.astype(F32)).astype(BF)
    return high, low


def contract_cols(left, right):
    return lax.dot_general(left, right, (((1,), (1,)), ((), ())), preferred_element_type=F32)


def matmul(left, right):
    return lax.dot_general(left, right, (((1,), (0,)), ((), ())), preferred_element_type=F32)


def ranks(routes):
    count = routes.shape[1]
    expert = iota((16, count), 0)
    first = routes[0:1, :] == expert
    second = routes[1:2, :] == expert
    member = jnp.where(first | second, 1.0, 0.0)
    before = one_if(iota((count, count), 0) < iota((count, count), 1))
    rank = matmul(member.astype(BF), before)
    return first, second, member, rank


def dispatch_kernel(
    routes_hbm, weights_hbm, tokens_ref, grad_ref, out_ref, data_ref, routes_ref, weights_ref, sems
):
    start = pl.multiple_of(lax.axis_index("tp") * 128, 128)
    small = [
        pltpu.make_async_copy(routes_hbm, routes_ref, sems.at[2]),
        pltpu.make_async_copy(weights_hbm, weights_ref, sems.at[3]),
    ]
    loads = [
        pltpu.make_async_copy(
            ref.at[:, pl.ds(start, 128)], data_ref.at[pl.ds(128 * k, 128), :], sems.at[k]
        )
        for k, ref in enumerate((tokens_ref, grad_ref))
    ]
    for load in small + loads:
        load.start()
    for load in small:
        load.wait()
    first, second, member, rank = ranks(routes_ref[...])
    weights = weights_ref[...]
    weight = jnp.where(first, weights[0:1, :], 0.0) + jnp.where(second, weights[1:2, :], 0.0)
    slot = jnp.where(member > 0.0, rank, -100.0).astype(jnp.int32)
    row = iota((16, PIECE, 128), 1)
    slot_3 = jnp.broadcast_to(slot[:, None, :], (16, PIECE, 128))
    sel_x = jnp.where(slot_3 == row, 1.0, 0.0)
    sel_dy = jnp.where(slot_3 + CAP == row, 1.0, 0.0)
    chosen = jnp.concatenate(
        [sel_x.reshape(16 * PIECE, 128).astype(BF), sel_dy.reshape(16 * PIECE, 128).astype(BF)], axis=1
    )
    value = jnp.sum(sel_x * weight[:, None, :], axis=2, keepdims=True)
    offset = (lax.axis_index("ep_0") % 4) * 32
    spread = jnp.where(iota((16, PIECE, 128), 2) == row + offset, value, 0.0)
    packed = jnp.sum(jnp.where(row < CAP, spread, 0.0), axis=1, keepdims=True)
    high = packed.astype(BF).astype(F32)
    low = packed - high
    for load in loads:
        load.wait()
    rows = matmul(chosen, data_ref[...]).reshape(16, PIECE, 128)
    rows = jnp.where(row == 36, high, jnp.where(row == 37, low, rows))
    out_ref[...] = rows.reshape(16 * PIECE, 128).astype(BF)


def plan_kernel(gate, up, down, copies_ref, swap_ref, sems):
    moves = [
        pltpu.make_async_copy(ref, swap_ref.at[pl.ds(2048 * k, 2048), :], sems.at[16 + k])
        for k, ref in enumerate((gate, up))
    ] + [
        pltpu.make_async_copy(
            down.at[:, pl.ds(128 * t, 128)], swap_ref.at[pl.ds(4096 + 128 * t, 128), :], sems.at[t]
        )
        for t in range(16)
    ]
    for move in moves:
        move.start()
    p = iota((2 * ROWS, 1), 0)
    is_dy = p >= ROWS
    q = jnp.where(is_dy, p - ROWS, p)
    source = (q * 3641) >> 16
    target = source * PIECE + (q - source * CAP) + jnp.where(is_dy, CAP, 0)
    copies_ref[0 : 2 * ROWS, :] = one_if(iota((2 * ROWS, SRC * PIECE), 1) == target)
    col = iota((16, SRC * PIECE), 1)
    of_source = (col * 1639) >> 16
    within = col - of_source * PIECE
    i = iota((16, SRC * PIECE), 0)
    pick = ((of_source >> 2) == (i & 3)) & (within == jnp.where(i >= 4, 37, 36)) & (i < 8)
    copies_ref[2 * ROWS : 2 * ROWS + 16, :] = one_if(pick)

    for move in moves:
        move.wait()


def places_kernel(routes_hbm, combine_ref, lanes_ref, routes_ref, sem):
    routes_load = pltpu.make_async_copy(routes_hbm, routes_ref, sem)
    routes_load.start()
    routes_load.wait()
    routes = routes_ref[...]
    first, second, member, rank = ranks(routes)
    slot = jnp.where(member > 0.0, rank, -100.0).astype(jnp.int32)
    row = iota((16, BACK, 128), 1)
    sel = jnp.where(jnp.broadcast_to(slot[:, None, :], (16, BACK, 128)) == row, 1.0, 0.0)
    combine_ref[0:128, :] = jnp.transpose(sel.reshape(16 * BACK, 128)).astype(BF)
    offset = (lax.axis_index("ep_0") % 4) * 32
    is_gate = (row == 18) | (row == 19)
    for k, mine in enumerate((first, second)):
        chosen = jnp.where(mine, 1.0, 0.0)[:, None, :]
        sel = jnp.where(is_gate, jnp.broadcast_to(chosen, (16, BACK, 128)), 0.0)
        combine_ref[128 * (k + 1) : 128 * (k + 2), :] = jnp.transpose(
            sel.reshape(16 * BACK, 128)
        ).astype(BF)
        index = jnp.sum(jnp.where(mine, rank, 0.0), axis=0, keepdims=True).astype(jnp.int32)
        lanes = jnp.where(iota((128, 128), 0) == index + offset, 1.0, 0.0)
        lanes_ref[128 * k : 128 * (k + 1), :] = jnp.transpose(lanes).astype(BF)


def copies_kernel(in_ref, pick_ref, out_ref):
    rows = matmul(pick_ref[...], in_ref[...]).astype(BF)
    for t in range(16):
        out_ref[t] = rows[:GATH]


def lane_of_row():
    r = iota((ROWS, 1), 0)
    source = (r * 3641) >> 16
    lane = (source & 3) * 32 + (r - source * CAP)
    return source >> 2, lane


def row_weights(extra):
    group, lane = lane_of_row()
    spread = matmul(one_if((iota((ROWS, 8), 1) & 3) == group), extra)
    return jnp.sum(jnp.where(iota((ROWS, 128), 1) == lane, spread, 0.0), axis=1, keepdims=True)


def pair_cols(ref, t, start):
    return jnp.concatenate([ref[2 * t, start : start + ROWS, :], ref[2 * t + 1, start : start + ROWS, :]], axis=1)


def main_kernel(own_ref, gate, up, down, swap_ref, part_ref, both_ref, hidden_ref):
    pre_gate = jnp.zeros((ROWS, 256), F32)
    pre_up = jnp.zeros((ROWS, 256), F32)
    d_hidden = jnp.zeros((ROWS, 256), F32)

    def both_halves(ref, t, first):
        cols = slice(256 * t, 256 * t + 256)
        return jnp.concatenate([ref[cols, :], swap_ref[first + 256 * t : first + 256 * t + 256, :]], axis=1)

    for t in range(8):
        x = pair_cols(own_ref, t, 0)
        pre_gate = pre_gate + matmul(x, both_halves(gate, t, 0))
        pre_up = pre_up + matmul(x, both_halves(up, t, 2048))
        at = 4096 + 256 * t
        down_2 = jnp.concatenate([swap_ref[at : at + 128, :], swap_ref[at + 128 : at + 256, :]], axis=1)
        d_hidden = d_hidden + contract_cols(
            pair_cols(own_ref, t, ROWS),
            jnp.concatenate([down[:, 256 * t : 256 * t + 256], down_2], axis=0),
        )
    sigma = jax.nn.sigmoid(pre_gate)
    activ = pre_gate * sigma
    hidden = activ * pre_up
    gate_part = jnp.sum(hidden * d_hidden, axis=1, keepdims=True)
    scaled = row_weights(own_ref[0, 2 * ROWS : GATH, :]) * d_hidden
    d_gate = (scaled * pre_up * sigma * (1.0 + pre_gate * (1.0 - sigma))).astype(BF)
    d_up = (scaled * activ).astype(BF)
    both_ref[:, 0:256] = d_gate
    both_ref[:, 256:512] = d_up
    hidden_ref[...] = hidden.astype(BF)
    _, lane = lane_of_row()
    spread = jnp.where(iota((ROWS, 128), 1) == lane, gate_part, 0.0)
    packed = jnp.sum(spread.reshape(4, ROWS // 4, 128), axis=1)
    extra = jnp.concatenate(split_two(packed), axis=0)
    for t in range(8):
        value = contract_cols(d_gate, both_halves(gate, t, 0))
        value = value + contract_cols(d_up, both_halves(up, t, 2048))
        value = value.astype(BF)
        for k in range(2):
            part_ref[2 * t + k, 0:ROWS, :] = value[:, 128 * k : 128 * k + 128]
            part_ref[2 * t + k, ROWS:PART, :] = extra


def half_grads(own_ref, both_ref, hidden_ref, half):
    lanes = slice(128 * half, 128 * half + 128)
    late = slice(256 + 128 * half, 256 + 128 * half + 128)
    both = jnp.concatenate([both_ref[:, lanes], both_ref[:, late]], axis=1)
    both_t = jnp.transpose(both.astype(F32)).astype(BF)
    hidden_t = jnp.transpose(hidden_ref[:, lanes].astype(F32)).astype(BF)
    g = row_weights(own_ref[0, 2 * ROWS : GATH, :])
    for t in range(8):
        cols = slice(256 * t, 256 * t + 256)
        scaled = (g * pair_cols(own_ref, t, ROWS).astype(F32)).astype(BF)
        yield cols, matmul(both_t, pair_cols(own_ref, t, 0)), matmul(hidden_t, scaled)


def partner_grads_kernel(own_ref, both_ref, hidden_ref, out_ref):
    for cols, both, down in half_grads(own_ref, both_ref, hidden_ref, 1):
        out_ref[0:256, cols] = both.astype(BF)
        out_ref[256:384, cols] = down.astype(BF)


def own_grads_kernel(own_ref, both_ref, hidden_ref, other_ref, gate_out, up_out, down_out):
    for cols, both, down in half_grads(own_ref, both_ref, hidden_ref, 0):
        grads = jnp.transpose(both + other_ref[0:256, cols].astype(F32))
        gate_out[cols, :] = grads[:, :128].astype(BF)
        up_out[cols, :] = grads[:, 128:].astype(BF)
        down_out[:, cols] = (down + other_ref[256:384, cols].astype(F32)).astype(BF)


def sum_kernel(in_ref, out_ref):
    rows = in_ref[0].astype(F32)
    for t in range(1, 16):
        rows = rows + in_ref[t].astype(F32)
    packed = rows[ROWS : ROWS + 4] + rows[ROWS + 4 : PART]
    high = packed.astype(BF).astype(F32)
    rows = jnp.concatenate([rows[:ROWS], high, packed - high], axis=0).astype(BF)
    p = iota((SRC * BACK, 1), 0)
    source = (p * 2731) >> 16
    j = p - source * BACK
    target = jnp.where(j < CAP, source * CAP + j, -1)
    target = jnp.where(j == 18, ROWS + (source >> 2), target)
    target = jnp.where(j == 19, ROWS + 4 + (source >> 2), target)
    pick = one_if(iota((SRC * BACK, PART), 1) == target)
    out_ref[...] = matmul(pick, rows).astype(BF)


def combine_kernel(in_ref, pick_ref, lanes_ref, tokens_ref, route_ref):
    values = matmul(pick_ref[...], in_ref[...])
    tokens_ref[...] = values[:128].astype(BF)
    gates = lax.dot_general(
        jnp.ones((8, 128), F32),
        values[128:] * lanes_ref[...].astype(F32),
        (((1,), (1,)), ((), ())),
        precision=lax.Precision.HIGHEST,
        preferred_element_type=F32,
    )
    route_ref[0:1, :] = gates[0:1, :128]
    route_ref[1:2, :] = gates[0:1, 128:]


def shape(dims, dtype=BF):
    return jax.ShapeDtypeStruct(dims, dtype)


def near(dims, dtype=BF):
    return pltpu.VMEM(dims, dtype)


def far(value):
    return pltpu.with_memory_space_constraint(value, pltpu.HBM)


def hold(value):
    return pltpu.with_memory_space_constraint(value, pltpu.VMEM)


def local(tokens, routes, route_weights, out_grad, gate_proj, up_proj, down_proj):
    return steps(tokens, routes, route_weights, out_grad, gate_proj[0], up_proj[0], down_proj[0])


def exchange(value, axis):
    return lax.all_to_all(value, axis, 0, 0, tiled=True)


def to_partner(value):
    return lax.ppermute(value, "ep_1", [(0, 1), (1, 0)])


def kernel(body, **settings):
    return pl.pallas_call(body, compiler_params=LIMIT, **settings)


def steps(tokens, routes, route_weights, out_grad, gate, up, down):
    count, width = tokens.shape
    routes_t = routes.T
    weights_t = route_weights.T
    vmem = pl.BlockSpec(memory_space=pltpu.VMEM)
    hbm = pl.BlockSpec(memory_space=pltpu.HBM)
    small = [pltpu.VMEM((2, count), jnp.int32), pltpu.VMEM((2, count), F32)]
    pieces = kernel(
        dispatch_kernel,
        in_specs=[hbm] * 4,
        out_shape=near((16 * PIECE, 128)),
        scratch_shapes=[pltpu.VMEM((256, 128), BF), *small, pltpu.SemaphoreType.DMA((4,))],
    )(far(routes_t), far(weights_t), far(tokens), far(out_grad))
    received = exchange(pieces.reshape(16, PIECE, 128), "ep_0")
    pick_copies, packed = kernel(
        plan_kernel,
        in_specs=[hbm] * 3,
        out_specs=(vmem, vmem),
        out_shape=(near((2 * ROWS + 16, SRC * PIECE)), near((3 * width, 128))),
        scratch_shapes=[pltpu.SemaphoreType.DMA((18,))],
    )(far(gate), far(up), far(down))
    packed_2 = to_partner(packed)
    received, packed_2 = lax.optimization_barrier((received, packed_2))
    copies = kernel(copies_kernel, out_shape=near((16, GATH, 128)))(
        hold(received.reshape(SRC * PIECE, 128)), hold(pick_copies)
    )
    own = hold(exchange(copies, "tp"))
    part, both, hidden = kernel(
        main_kernel,
        in_specs=[vmem] * 5,
        out_specs=(vmem, vmem, vmem),
        out_shape=(near((16, PART, 128)), near((ROWS, 512)), near((ROWS, 256))),
    )(own, gate, up, down, hold(packed_2))
    spread = exchange(part, "tp")
    partner = kernel(partner_grads_kernel, out_shape=shape((384, width)))(own, both, hidden)
    mine = to_partner(partner)
    gate_grad, up_grad, down_grad = kernel(
        own_grads_kernel, out_shape=(shape((width, 128)), shape((width, 128)), shape((128, width)))
    )(own, both, hidden, mine)
    back = kernel(sum_kernel, out_shape=near((SRC * BACK, 128)))(hold(spread))
    pick_combine, lanes = kernel(
        places_kernel,
        in_specs=[hbm],
        out_specs=(vmem, vmem),
        out_shape=(near((384, 16 * BACK)), near((256, 128))),
        scratch_shapes=[small[0], pltpu.SemaphoreType.DMA],
    )(far(routes_t))
    home = exchange(back.reshape(SRC, BACK, 128), "ep_0")
    tokens_grad, route_grad = kernel(
        combine_kernel, out_shape=(shape((count, 128)), shape((2, count), F32))
    )(hold(home.reshape(16 * BACK, 128)), hold(pick_combine), hold(lanes))
    return (tokens_grad, route_grad.T, gate_grad[None], up_grad[None], down_grad[None])


def solution(mesh):
    torus = Mesh(mesh.devices.reshape(16, 2, mesh.shape["tp"]), ("ep_0", "ep_1", "tp"))
    placed = (
        P(EP, None),
        P(EP, None),
        P(EP, None),
        P(EP, None),
        P(EP, None, "tp"),
        P(EP, None, "tp"),
        P(EP, "tp", None),
    )
    return jax.shard_map(
        local,
        mesh=torus,
        in_specs=placed,
        out_specs=(
            P(EP, "tp"),
            P(EP, None),
            P(EP, None, "tp"),
            P(EP, None, "tp"),
            P(EP, "tp", None),
        ),
        check_vma=False,
    )
```

```python
import jax
import jax.numpy as jnp
from jax import lax
from jax.experimental import pallas as pl
from jax.experimental.pallas import tpu as pltpu
from jax.sharding import Mesh
from jax.sharding import PartitionSpec as P


EP = ("ep_0", "ep_1")
BF = jnp.bfloat16
F32 = jnp.float32

CAP = 18
SRC = 16
ROWS = SRC * CAP
PIECE = 36
BACK = 20
GATH = 2 * ROWS
PART = ROWS + 8
LIMIT = pltpu.CompilerParams(vmem_limit_bytes=24 * 1024 * 1024)


def iota(shape, dim):
    return lax.broadcasted_iota(jnp.int32, shape, dim)


def one_if(cond):
    return jnp.where(cond, 1.0, 0.0).astype(BF)


def split_two(value):
    high = value.astype(BF)
    low = (value - high.astype(F32)).astype(BF)
    return high, low


def contract_cols(left, right):
    return lax.dot_general(left, right, (((1,), (1,)), ((), ())), preferred_element_type=F32)


def matmul(left, right):
    return lax.dot_general(left, right, (((1,), (0,)), ((), ())), preferred_element_type=F32)


def expand(expert, values):
    return matmul(one_if(iota((expert.shape[0], 16), 1) == expert), values)


def ranks(routes):
    count = routes.shape[1]
    expert = iota((16, count), 0)
    first = routes[0:1, :] == expert
    second = routes[1:2, :] == expert
    member = jnp.where(first | second, 1.0, 0.0)
    before = one_if(iota((count, count), 0) < iota((count, count), 1))
    rank = matmul(member.astype(BF), before)
    return first, second, member, rank


def dispatch_kernel(
    routes_hbm, weights_hbm, tokens_ref, grad_ref, out_ref, data_ref, routes_ref, weights_ref, sems
):
    start = pl.multiple_of(lax.axis_index("tp") * 128, 128)
    small = [
        pltpu.make_async_copy(routes_hbm, routes_ref, sems.at[2]),
        pltpu.make_async_copy(weights_hbm, weights_ref, sems.at[3]),
    ]
    loads = [
        pltpu.make_async_copy(
            ref.at[:, pl.ds(start, 128)], data_ref.at[pl.ds(128 * k, 128), :], sems.at[k]
        )
        for k, ref in enumerate((tokens_ref, grad_ref))
    ]
    for load in small + loads:
        load.start()
    for load in small:
        load.wait()
    first, second, member, rank = ranks(routes_ref[...])
    weights = weights_ref[...]
    weight = jnp.where(first, weights[0:1, :], 0.0) + jnp.where(second, weights[1:2, :], 0.0)
    slot = jnp.where(member > 0.0, rank, -100.0)
    row = iota((16 * PIECE, 1), 0)
    expert = (row * 1821) >> 16
    slots = expand(expert, slot.astype(BF)).astype(jnp.int32)
    within = row - expert * PIECE
    sel_x = slots == within
    sel_dy = slots + CAP == within
    high, low = split_two(weight)
    lowest = (weight - high.astype(F32) - low.astype(F32)).astype(BF)
    spread = expand(expert, high) + expand(expert, low) + expand(expert, lowest)
    factor = jnp.sum(jnp.where(sel_dy, spread, 0.0), axis=1, keepdims=True)
    factor = jnp.where(within < CAP, 1.0, factor)
    chosen = jnp.concatenate([one_if(sel_x), one_if(sel_dy)], axis=1)
    for load in loads:
        load.wait()
    out_ref[...] = (matmul(chosen, data_ref[...]) * factor).astype(BF)


def plan_kernel(gate, up, down, copies_ref, swap_ref, sems):
    moves = [
        pltpu.make_async_copy(ref, swap_ref.at[pl.ds(2048 * k, 2048), :], sems.at[16 + k])
        for k, ref in enumerate((gate, up))
    ] + [
        pltpu.make_async_copy(
            down.at[:, pl.ds(128 * t, 128)], swap_ref.at[pl.ds(4096 + 128 * t, 128), :], sems.at[t]
        )
        for t in range(16)
    ]
    for move in moves:
        move.start()
    p = iota((GATH, 1), 0)
    is_dy = p >= ROWS
    q = jnp.where(is_dy, p - ROWS, p)
    source = (q * 3641) >> 16
    target = source * PIECE + (q - source * CAP) + jnp.where(is_dy, CAP, 0)
    copies_ref[...] = one_if(iota((GATH, SRC * PIECE), 1) == target)
    for move in moves:
        move.wait()


def places_kernel(routes_hbm, weights_hbm, combine_ref, lanes_ref, routes_ref, weights_ref, sems):
    loads = [
        pltpu.make_async_copy(routes_hbm, routes_ref, sems.at[0]),
        pltpu.make_async_copy(weights_hbm, weights_ref, sems.at[1]),
    ]
    for load in loads:
        load.start()
    for load in loads:
        load.wait()
    routes = routes_ref[...]
    first, second, member, rank = ranks(routes)
    slot = jnp.where(member > 0.0, rank, -100.0)
    row = iota((16 * BACK, 1), 0)
    expert = (row * 3277) >> 16
    within = row - expert * BACK
    sel = jnp.where(expand(expert, slot.astype(BF)).astype(jnp.int32) == within, 1.0, 0.0)
    combine_ref[0:128, :] = jnp.transpose(sel).astype(BF)
    offset = (lax.axis_index("ep_0") % 4) * 32
    weights = weights_ref[...]
    for k, mine in enumerate((first, second)):
        sel = jnp.where(within >= CAP, expand(expert, one_if(mine)), 0.0)
        combine_ref[128 * (k + 1) : 128 * (k + 2), :] = jnp.transpose(sel).astype(BF)
        index = jnp.sum(jnp.where(mine, rank, 0.0), axis=0, keepdims=True).astype(jnp.int32)
        lanes = jnp.where(iota((128, 128), 0) == index + offset, 1.0 / weights[k : k + 1, :], 0.0)
        lanes_ref[128 * k : 128 * (k + 1), :] = jnp.transpose(lanes)


def settle_kernel(in_ref, out_ref):
    del in_ref, out_ref


def copies_kernel(in_ref, pick_ref, out_ref):
    rows = matmul(pick_ref[...], in_ref[...]).astype(BF)
    for t in range(16):
        out_ref[t] = rows


def lane_of_row():
    r = iota((ROWS, 1), 0)
    source = (r * 3641) >> 16
    lane = (source & 3) * 32 + (r - source * CAP)
    return source >> 2, lane


def pair_cols(ref, t, start):
    return jnp.concatenate([ref[2 * t, start : start + ROWS, :], ref[2 * t + 1, start : start + ROWS, :]], axis=1)


def main_kernel(own_ref, gate, up, down, swap_ref, part_ref, both_ref, hidden_ref):
    pre_gate = jnp.zeros((ROWS, 256), F32)
    pre_up = jnp.zeros((ROWS, 256), F32)
    d_hidden = jnp.zeros((ROWS, 256), F32)

    def both_halves(ref, t, first):
        cols = slice(256 * t, 256 * t + 256)
        return jnp.concatenate([ref[cols, :], swap_ref[first + 256 * t : first + 256 * t + 256, :]], axis=1)

    for t in range(8):
        x = pair_cols(own_ref, t, 0)
        pre_gate = pre_gate + matmul(x, both_halves(gate, t, 0))
        pre_up = pre_up + matmul(x, both_halves(up, t, 2048))
        at = 4096 + 256 * t
        down_2 = jnp.concatenate([swap_ref[at : at + 128, :], swap_ref[at + 128 : at + 256, :]], axis=1)
        d_hidden = d_hidden + contract_cols(
            pair_cols(own_ref, t, ROWS),
            jnp.concatenate([down[:, 256 * t : 256 * t + 256], down_2], axis=0),
        )
    sigma = jax.nn.sigmoid(pre_gate)
    activ = pre_gate * sigma
    hidden = activ * pre_up
    gate_part = jnp.sum(hidden * d_hidden, axis=1, keepdims=True)
    d_gate = (d_hidden * pre_up * sigma * (1.0 + pre_gate * (1.0 - sigma))).astype(BF)
    d_up = (d_hidden * activ).astype(BF)
    both_ref[:, 0:256] = d_gate
    both_ref[:, 256:512] = d_up
    hidden_ref[...] = hidden.astype(BF)
    _, lane = lane_of_row()
    spread = jnp.where(iota((ROWS, 128), 1) == lane, gate_part, 0.0)
    packed = jnp.sum(spread.reshape(4, ROWS // 4, 128), axis=1)
    extra = jnp.concatenate(split_two(packed), axis=0)
    for t in range(8):
        value = contract_cols(d_gate, both_halves(gate, t, 0))
        value = value + contract_cols(d_up, both_halves(up, t, 2048))
        value = value.astype(BF)
        for k in range(2):
            part_ref[2 * t + k, 0:ROWS, :] = value[:, 128 * k : 128 * k + 128]
            part_ref[2 * t + k, ROWS:PART, :] = extra


def half_grads(own_ref, both_ref, hidden_ref, half):
    lanes = slice(128 * half, 128 * half + 128)
    late = slice(256 + 128 * half, 256 + 128 * half + 128)
    both = jnp.concatenate([both_ref[:, lanes], both_ref[:, late]], axis=1)
    both_t = jnp.transpose(both.astype(F32)).astype(BF)
    hidden_t = jnp.transpose(hidden_ref[:, lanes].astype(F32)).astype(BF)
    for t in range(8):
        cols = slice(256 * t, 256 * t + 256)
        grads = matmul(both_t, pair_cols(own_ref, t, 0))
        yield cols, grads, matmul(hidden_t, pair_cols(own_ref, t, ROWS))


def partner_grads_kernel(own_ref, both_ref, hidden_ref, out_ref):
    for cols, both, down in half_grads(own_ref, both_ref, hidden_ref, 1):
        out_ref[0:256, cols] = both.astype(BF)
        out_ref[256:384, cols] = down.astype(BF)


def own_grads_kernel(own_ref, both_ref, hidden_ref, other_ref, gate_out, up_out, down_out):
    for cols, both, down in half_grads(own_ref, both_ref, hidden_ref, 0):
        grads = jnp.transpose(both + other_ref[0:256, cols].astype(F32))
        gate_out[cols, :] = grads[:, :128].astype(BF)
        up_out[cols, :] = grads[:, 128:].astype(BF)
        down_out[:, cols] = (down + other_ref[256:384, cols].astype(F32)).astype(BF)


def sum_kernel(in_ref, out_ref):
    rows = in_ref[0].astype(F32)
    for t in range(1, 16):
        rows = rows + in_ref[t].astype(F32)
    packed = rows[ROWS : ROWS + 4] + rows[ROWS + 4 : PART]
    high = packed.astype(BF).astype(F32)
    rows = jnp.concatenate([rows[:ROWS], high, packed - high], axis=0).astype(BF)
    p = iota((SRC * BACK, 1), 0)
    source = (p * 3277) >> 16
    j = p - source * BACK
    target = jnp.where(j < CAP, source * CAP + j, -1)
    target = jnp.where(j == 18, ROWS + (source >> 2), target)
    target = jnp.where(j == 19, ROWS + 4 + (source >> 2), target)
    pick = one_if(iota((SRC * BACK, PART), 1) == target)
    out_ref[...] = matmul(pick, rows).astype(BF)


def combine_kernel(in_ref, pick_ref, lanes_ref, tokens_ref, route_ref):
    values = matmul(pick_ref[...], in_ref[...])
    tokens_ref[...] = values[:128].astype(BF)
    gates = lax.dot_general(
        jnp.ones((8, 128), F32),
        values[128:] * lanes_ref[...],
        (((1,), (1,)), ((), ())),
        precision=lax.Precision.HIGHEST,
        preferred_element_type=F32,
    )
    route_ref[0:1, :] = gates[0:1, :128]
    route_ref[1:2, :] = gates[0:1, 128:]


def shape(dims, dtype=BF):
    return jax.ShapeDtypeStruct(dims, dtype)


def far_shape(dims, dtype=BF):
    return pltpu.HBM(dims, dtype)


def near(dims, dtype=BF):
    return pltpu.VMEM(dims, dtype)


def far(value):
    return pltpu.with_memory_space_constraint(value, pltpu.HBM)


def hold(value):
    return pltpu.with_memory_space_constraint(value, pltpu.VMEM)


def local(tokens, routes, route_weights, out_grad, gate_proj, up_proj, down_proj):
    return steps(tokens, routes, route_weights, out_grad, gate_proj[0], up_proj[0], down_proj[0])


def exchange(value, axis):
    return lax.all_to_all(value, axis, 0, 0, tiled=True)


def to_partner(value):
    return lax.ppermute(value, "ep_1", [(0, 1), (1, 0)])


def kernel(body, **settings):
    return pl.pallas_call(body, compiler_params=LIMIT, **settings)


def steps(tokens, routes, route_weights, out_grad, gate, up, down):
    count, width = tokens.shape
    routes_t = routes.T
    weights_t = route_weights.T
    vmem = pl.BlockSpec(memory_space=pltpu.VMEM)
    hbm = pl.BlockSpec(memory_space=pltpu.HBM)
    small = [pltpu.VMEM((2, count), jnp.int32), pltpu.VMEM((2, count), F32)]
    pieces = kernel(
        dispatch_kernel,
        in_specs=[hbm] * 4,
        out_shape=near((16 * PIECE, 128)),
        scratch_shapes=[pltpu.VMEM((256, 128), BF), *small, pltpu.SemaphoreType.DMA((4,))],
    )(far(routes_t), far(weights_t), far(tokens), far(out_grad))
    received = exchange(pieces.reshape(16, PIECE // 4, 4, 128), "ep_0")
    pick_copies, packed = kernel(
        plan_kernel,
        in_specs=[hbm] * 3,
        out_specs=(vmem, vmem),
        out_shape=(near((GATH, SRC * PIECE)), near((3 * width, 128))),
        scratch_shapes=[pltpu.SemaphoreType.DMA((18,))],
    )(far(gate), far(up), far(down))
    packed_2 = to_partner(packed)
    packed_2 = kernel(
        settle_kernel,
        in_specs=[hbm],
        out_specs=hbm,
        out_shape=far_shape((3 * width, 128)),
        input_output_aliases={0: 0},
    )(far(packed_2))
    copies = kernel(copies_kernel, out_shape=near((16, GATH, 128)))(
        hold(received.reshape(SRC * PIECE, 128)), hold(pick_copies)
    )
    own = hold(exchange(copies, "tp"))
    part, both, hidden = kernel(
        main_kernel,
        in_specs=[vmem] * 5,
        out_specs=(vmem, vmem, vmem),
        out_shape=(near((16, PART, 128)), near((ROWS, 512)), near((ROWS, 256))),
    )(own, gate, up, down, packed_2)
    spread = exchange(part, "tp")
    partner = kernel(partner_grads_kernel, out_shape=shape((384, width)))(own, both, hidden)
    mine = to_partner(partner)
    gate_grad, up_grad, down_grad = kernel(
        own_grads_kernel, out_shape=(shape((width, 128)), shape((width, 128)), shape((128, width)))
    )(own, both, hidden, mine)
    back = kernel(sum_kernel, out_shape=near((SRC * BACK, 128)))(hold(spread))
    pick_combine, lanes = kernel(
        places_kernel,
        in_specs=[hbm] * 2,
        out_specs=(vmem, vmem),
        out_shape=(near((384, 16 * BACK)), near((256, 128), F32)),
        scratch_shapes=[*small, pltpu.SemaphoreType.DMA((2,))],
    )(far(routes_t), far(weights_t))
    home = exchange(back.reshape(SRC, BACK // 4, 4, 128), "ep_0")
    tokens_grad, route_grad = kernel(
        combine_kernel, out_shape=(shape((count, 128)), shape((2, count), F32))
    )(hold(home.reshape(16 * BACK, 128)), hold(pick_combine), hold(lanes))
    return (tokens_grad, route_grad.T, gate_grad[None], up_grad[None], down_grad[None])


def solution(mesh):
    torus = Mesh(mesh.devices.reshape(16, 2, mesh.shape["tp"]), ("ep_0", "ep_1", "tp"))
    placed = (
        P(EP, None),
        P(EP, None),
        P(EP, None),
        P(EP, None),
        P(EP, None, "tp"),
        P(EP, None, "tp"),
        P(EP, "tp", None),
    )
    return jax.shard_map(
        local,
        mesh=torus,
        in_specs=placed,
        out_specs=(
            P(EP, "tp"),
            P(EP, None),
            P(EP, None, "tp"),
            P(EP, None, "tp"),
            P(EP, "tp", None),
        ),
        check_vma=False,
    )
```

```python
import jax
import jax.numpy as jnp
from jax import lax
from jax.experimental import pallas as pl
from jax.experimental.pallas import tpu as pltpu
from jax.sharding import Mesh
from jax.sharding import PartitionSpec as P


EP = ("ep_0", "ep_1")
BF = jnp.bfloat16
F32 = jnp.float32

CAP = 18
SRC = 16
ROWS = SRC * CAP
PIECE = 36
BACK = 20
GATH = 2 * ROWS
PART = ROWS + 8
LIMIT = pltpu.CompilerParams(vmem_limit_bytes=24 * 1024 * 1024)


def iota(shape, dim):
    return lax.broadcasted_iota(jnp.int32, shape, dim)


def one_if(cond):
    return jnp.where(cond, 1.0, 0.0).astype(BF)


def split_two(value):
    high = value.astype(BF)
    low = (value - high.astype(F32)).astype(BF)
    return high, low


def contract_cols(left, right):
    return lax.dot_general(left, right, (((1,), (1,)), ((), ())), preferred_element_type=F32)


def matmul(left, right):
    return lax.dot_general(left, right, (((1,), (0,)), ((), ())), preferred_element_type=F32)


def member_at(place):
    return jnp.where((place & 1) == 1, (9 + (place >> 1)) & 15, 8 - (place >> 1))


def own_lanes():
    z = lax.axis_index("ep_0")
    place = jnp.where(z == 0, 15, jnp.where(z < 9, 16 - 2 * z, 2 * z - 17))
    return (place % 4) * 32


def expand(expert, values):
    return matmul(one_if(iota((expert.shape[0], 16), 1) == expert), values)


def ranks(routes):
    count = routes.shape[1]
    expert = iota((16, count), 0)
    first = routes[0:1, :] == expert
    second = routes[1:2, :] == expert
    member = jnp.where(first | second, 1.0, 0.0)
    before = one_if(iota((count, count), 0) < iota((count, count), 1))
    rank = matmul(member.astype(BF), before)
    return first, second, member, rank


def dispatch_kernel(
    routes_hbm, weights_hbm, tokens_ref, grad_ref, out_ref, data_ref, routes_ref, weights_ref, sems
):
    start = pl.multiple_of(lax.axis_index("tp") * 128, 128)
    small = [
        pltpu.make_async_copy(routes_hbm, routes_ref, sems.at[2]),
        pltpu.make_async_copy(weights_hbm, weights_ref, sems.at[3]),
    ]
    loads = [
        pltpu.make_async_copy(
            ref.at[:, pl.ds(start, 128)], data_ref.at[pl.ds(128 * k, 128), :], sems.at[k]
        )
        for k, ref in enumerate((tokens_ref, grad_ref))
    ]
    for load in small + loads:
        load.start()
    for load in small:
        load.wait()
    first, second, member, rank = ranks(routes_ref[...])
    weights = weights_ref[...]
    weight = jnp.where(first, weights[0:1, :], 0.0) + jnp.where(second, weights[1:2, :], 0.0)
    slot = jnp.where(member > 0.0, rank, -100.0)
    row = iota((16 * PIECE, 1), 0)
    place = (row * 1821) >> 16
    expert = member_at(place)
    slots = expand(expert, slot.astype(BF)).astype(jnp.int32)
    within = row - place * PIECE
    sel_x = slots == within
    sel_dy = slots + CAP == within
    high, low = split_two(weight)
    lowest = (weight - high.astype(F32) - low.astype(F32)).astype(BF)
    spread = expand(expert, high) + expand(expert, low) + expand(expert, lowest)
    factor = jnp.sum(jnp.where(sel_dy, spread, 0.0), axis=1, keepdims=True)
    factor = jnp.where(within < CAP, 1.0, factor)
    chosen = jnp.concatenate([one_if(sel_x), one_if(sel_dy)], axis=1)
    for load in loads:
        load.wait()
    out_ref[...] = (matmul(chosen, data_ref[...]) * factor).astype(BF)


def plan_kernel(gate, up, down, copies_ref, swap_ref, sems):
    moves = [
        pltpu.make_async_copy(ref, swap_ref.at[pl.ds(2048 * k, 2048), :], sems.at[16 + k])
        for k, ref in enumerate((gate, up))
    ] + [
        pltpu.make_async_copy(
            down.at[:, pl.ds(128 * t, 128)], swap_ref.at[pl.ds(4096 + 128 * t, 128), :], sems.at[t]
        )
        for t in range(16)
    ]
    for move in moves:
        move.start()
    p = iota((GATH, 1), 0)
    is_dy = p >= ROWS
    q = jnp.where(is_dy, p - ROWS, p)
    source = (q * 3641) >> 16
    target = source * PIECE + (q - source * CAP) + jnp.where(is_dy, CAP, 0)
    copies_ref[...] = one_if(iota((GATH, SRC * PIECE), 1) == target)
    for move in moves:
        move.wait()


def places_kernel(routes_hbm, weights_hbm, combine_ref, lanes_ref, routes_ref, weights_ref, sems):
    loads = [
        pltpu.make_async_copy(routes_hbm, routes_ref, sems.at[0]),
        pltpu.make_async_copy(weights_hbm, weights_ref, sems.at[1]),
    ]
    for load in loads:
        load.start()
    for load in loads:
        load.wait()
    routes = routes_ref[...]
    first, second, member, rank = ranks(routes)
    slot = jnp.where(member > 0.0, rank, -100.0)
    row = iota((16 * BACK, 1), 0)
    place = (row * 3277) >> 16
    expert = member_at(place)
    within = row - place * BACK
    sel = jnp.where(expand(expert, slot.astype(BF)).astype(jnp.int32) == within, 1.0, 0.0)
    combine_ref[0:128, :] = jnp.transpose(sel).astype(BF)
    offset = own_lanes()
    weights = weights_ref[...]
    for k, mine in enumerate((first, second)):
        sel = jnp.where(within >= CAP, expand(expert, one_if(mine)), 0.0)
        combine_ref[128 * (k + 1) : 128 * (k + 2), :] = jnp.transpose(sel).astype(BF)
        index = jnp.sum(jnp.where(mine, rank, 0.0), axis=0, keepdims=True).astype(jnp.int32)
        lanes = jnp.where(iota((128, 128), 0) == index + offset, 1.0 / weights[k : k + 1, :], 0.0)
        lanes_ref[128 * k : 128 * (k + 1), :] = jnp.transpose(lanes)


def settle_kernel(in_ref, out_ref):
    del in_ref, out_ref


def copies_kernel(in_ref, pick_ref, out_ref):
    rows = matmul(pick_ref[...], in_ref[...]).astype(BF)
    for t in range(16):
        out_ref[t] = rows


def lane_of_row():
    r = iota((ROWS, 1), 0)
    source = (r * 3641) >> 16
    lane = (source & 3) * 32 + (r - source * CAP)
    return source >> 2, lane


def pair_cols(ref, t, start):
    return jnp.concatenate([ref[2 * t, start : start + ROWS, :], ref[2 * t + 1, start : start + ROWS, :]], axis=1)


def main_kernel(own_ref, gate, up, down, swap_ref, part_ref, both_ref, hidden_ref):
    pre_gate = jnp.zeros((ROWS, 256), F32)
    pre_up = jnp.zeros((ROWS, 256), F32)
    d_hidden = jnp.zeros((ROWS, 256), F32)

    def both_halves(ref, t, first):
        cols = slice(256 * t, 256 * t + 256)
        return jnp.concatenate([ref[cols, :], swap_ref[first + 256 * t : first + 256 * t + 256, :]], axis=1)

    for t in range(8):
        x = pair_cols(own_ref, t, 0)
        pre_gate = pre_gate + matmul(x, both_halves(gate, t, 0))
        pre_up = pre_up + matmul(x, both_halves(up, t, 2048))
        at = 4096 + 256 * t
        down_2 = jnp.concatenate([swap_ref[at : at + 128, :], swap_ref[at + 128 : at + 256, :]], axis=1)
        d_hidden = d_hidden + contract_cols(
            pair_cols(own_ref, t, ROWS),
            jnp.concatenate([down[:, 256 * t : 256 * t + 256], down_2], axis=0),
        )
    sigma = jax.nn.sigmoid(pre_gate)
    activ = pre_gate * sigma
    hidden = activ * pre_up
    gate_part = jnp.sum(hidden * d_hidden, axis=1, keepdims=True)
    d_gate = (d_hidden * pre_up * sigma * (1.0 + pre_gate * (1.0 - sigma))).astype(BF)
    d_up = (d_hidden * activ).astype(BF)
    both_ref[:, 0:256] = d_gate
    both_ref[:, 256:512] = d_up
    hidden_ref[...] = hidden.astype(BF)
    _, lane = lane_of_row()
    spread = jnp.where(iota((ROWS, 128), 1) == lane, gate_part, 0.0)
    packed = jnp.sum(spread.reshape(4, ROWS // 4, 128), axis=1)
    extra = jnp.concatenate(split_two(packed), axis=0)
    for t in range(8):
        value = contract_cols(d_gate, both_halves(gate, t, 0))
        value = value + contract_cols(d_up, both_halves(up, t, 2048))
        value = value.astype(BF)
        for k in range(2):
            part_ref[2 * t + k, 0:ROWS, :] = value[:, 128 * k : 128 * k + 128]
            part_ref[2 * t + k, ROWS:PART, :] = extra


def half_grads(own_ref, both_ref, hidden_ref, half):
    lanes = slice(128 * half, 128 * half + 128)
    late = slice(256 + 128 * half, 256 + 128 * half + 128)
    both = jnp.concatenate([both_ref[:, lanes], both_ref[:, late]], axis=1)
    both_t = jnp.transpose(both.astype(F32)).astype(BF)
    hidden_t = jnp.transpose(hidden_ref[:, lanes].astype(F32)).astype(BF)
    for t in range(8):
        cols = slice(256 * t, 256 * t + 256)
        grads = matmul(both_t, pair_cols(own_ref, t, 0))
        yield cols, grads, matmul(hidden_t, pair_cols(own_ref, t, ROWS))


def partner_grads_kernel(own_ref, both_ref, hidden_ref, out_ref):
    for cols, both, down in half_grads(own_ref, both_ref, hidden_ref, 1):
        out_ref[0:256, cols] = both.astype(BF)
        out_ref[256:384, cols] = down.astype(BF)


def own_grads_kernel(own_ref, both_ref, hidden_ref, other_ref, gate_out, up_out, down_out):
    for cols, both, down in half_grads(own_ref, both_ref, hidden_ref, 0):
        grads = jnp.transpose(both + other_ref[0:256, cols].astype(F32))
        gate_out[cols, :] = grads[:, :128].astype(BF)
        up_out[cols, :] = grads[:, 128:].astype(BF)
        down_out[:, cols] = (down + other_ref[256:384, cols].astype(F32)).astype(BF)


def sum_kernel(in_ref, out_ref):
    rows = in_ref[0].astype(F32)
    for t in range(1, 16):
        rows = rows + in_ref[t].astype(F32)
    packed = rows[ROWS : ROWS + 4] + rows[ROWS + 4 : PART]
    high = packed.astype(BF).astype(F32)
    rows = jnp.concatenate([rows[:ROWS], high, packed - high], axis=0).astype(BF)
    p = iota((SRC * BACK, 1), 0)
    source = (p * 3277) >> 16
    j = p - source * BACK
    target = jnp.where(j < CAP, source * CAP + j, -1)
    target = jnp.where(j == 18, ROWS + (source >> 2), target)
    target = jnp.where(j == 19, ROWS + 4 + (source >> 2), target)
    pick = one_if(iota((SRC * BACK, PART), 1) == target)
    out_ref[...] = matmul(pick, rows).astype(BF)


def combine_kernel(in_ref, pick_ref, lanes_ref, tokens_ref, route_ref):
    values = matmul(pick_ref[...], in_ref[...])
    tokens_ref[...] = values[:128].astype(BF)
    gates = lax.dot_general(
        jnp.ones((8, 128), F32),
        values[128:] * lanes_ref[...],
        (((1,), (1,)), ((), ())),
        precision=lax.Precision.HIGHEST,
        preferred_element_type=F32,
    )
    route_ref[0:1, :] = gates[0:1, :128]
    route_ref[1:2, :] = gates[0:1, 128:]


def shape(dims, dtype=BF):
    return jax.ShapeDtypeStruct(dims, dtype)


def far_shape(dims, dtype=BF):
    return pltpu.HBM(dims, dtype)


def near(dims, dtype=BF):
    return pltpu.VMEM(dims, dtype)


def far(value):
    return pltpu.with_memory_space_constraint(value, pltpu.HBM)


def hold(value):
    return pltpu.with_memory_space_constraint(value, pltpu.VMEM)


def local(tokens, routes, route_weights, out_grad, gate_proj, up_proj, down_proj):
    return steps(tokens, routes, route_weights, out_grad, gate_proj[0], up_proj[0], down_proj[0])


def exchange(value, axis):
    groups = [[8 - k // 2 if k % 2 == 0 else (9 + k // 2) % 16 for k in range(16)]] if axis == "ep_0" else None
    return lax.all_to_all(value, axis, 0, 0, axis_index_groups=groups, tiled=True)


def to_partner(value):
    return lax.ppermute(value, "ep_1", [(0, 1), (1, 0)])


def kernel(body, **settings):
    return pl.pallas_call(body, compiler_params=LIMIT, **settings)


def steps(tokens, routes, route_weights, out_grad, gate, up, down):
    count, width = tokens.shape
    routes_t = routes.T
    weights_t = route_weights.T
    vmem = pl.BlockSpec(memory_space=pltpu.VMEM)
    hbm = pl.BlockSpec(memory_space=pltpu.HBM)
    small = [pltpu.VMEM((2, count), jnp.int32), pltpu.VMEM((2, count), F32)]
    pieces = kernel(
        dispatch_kernel,
        in_specs=[hbm] * 4,
        out_shape=near((16 * PIECE, 128)),
        scratch_shapes=[pltpu.VMEM((256, 128), BF), *small, pltpu.SemaphoreType.DMA((4,))],
    )(far(routes_t), far(weights_t), far(tokens), far(out_grad))
    received = exchange(pieces.reshape(16, PIECE // 4, 4, 128), "ep_0")
    pick_copies, packed = kernel(
        plan_kernel,
        in_specs=[hbm] * 3,
        out_specs=(vmem, vmem),
        out_shape=(near((GATH, SRC * PIECE)), near((3 * width, 128))),
        scratch_shapes=[pltpu.SemaphoreType.DMA((18,))],
    )(far(gate), far(up), far(down))
    packed_2 = to_partner(packed)
    packed_2 = kernel(
        settle_kernel,
        in_specs=[hbm],
        out_specs=hbm,
        out_shape=far_shape((3 * width, 128)),
        input_output_aliases={0: 0},
    )(far(packed_2))
    copies = kernel(copies_kernel, out_shape=near((16, GATH, 128)))(
        hold(received.reshape(SRC * PIECE, 128)), hold(pick_copies)
    )
    gathered = exchange(copies, "tp")
    own, own_far = hold(gathered), far(gathered)
    part, both, hidden = kernel(
        main_kernel,
        in_specs=[vmem] * 5,
        out_specs=(vmem, vmem, vmem),
        out_shape=(near((16, PART, 128)), near((ROWS, 512)), near((ROWS, 256))),
    )(own, gate, up, down, packed_2)
    spread = exchange(part, "tp")
    partner = kernel(partner_grads_kernel, out_shape=shape((384, width)))(own_far, both, hidden)
    mine = to_partner(partner)
    gate_grad, up_grad, down_grad = kernel(
        own_grads_kernel, out_shape=(shape((width, 128)), shape((width, 128)), shape((128, width)))
    )(own_far, both, hidden, mine)
    back = kernel(sum_kernel, out_shape=near((SRC * BACK, 128)))(hold(spread))
    pick_combine, lanes = kernel(
        places_kernel,
        in_specs=[hbm] * 2,
        out_specs=(vmem, vmem),
        out_shape=(near((384, 16 * BACK)), near((256, 128), F32)),
        scratch_shapes=[*small, pltpu.SemaphoreType.DMA((2,))],
    )(far(routes_t), far(weights_t))
    home = exchange(back.reshape(SRC, BACK // 4, 4, 128), "ep_0")
    tokens_grad, route_grad = kernel(
        combine_kernel, out_shape=(shape((count, 128)), shape((2, count), F32))
    )(hold(home.reshape(16 * BACK, 128)), hold(pick_combine), hold(lanes))
    return (tokens_grad, route_grad.T, gate_grad[None], up_grad[None], down_grad[None])


def solution(mesh):
    torus = Mesh(mesh.devices.reshape(16, 2, mesh.shape["tp"]), ("ep_0", "ep_1", "tp"))
    placed = (
        P(EP, None),
        P(EP, None),
        P(EP, None),
        P(EP, None),
        P(EP, None, "tp"),
        P(EP, None, "tp"),
        P(EP, "tp", None),
    )
    return jax.shard_map(
        local,
        mesh=torus,
        in_specs=placed,
        out_specs=(
            P(EP, "tp"),
            P(EP, None),
            P(EP, None, "tp"),
            P(EP, None, "tp"),
            P(EP, "tp", None),
        ),
        check_vma=False,
    )
```

```python
import jax
import jax.numpy as jnp
from jax import lax
from jax.experimental import pallas as pl
from jax.experimental.pallas import tpu as pltpu
from jax.sharding import Mesh
from jax.sharding import PartitionSpec as P


EP = ("ep_0", "ep_1")
BF = jnp.bfloat16
F32 = jnp.float32

CAP = 18
SRC = 16
ROWS = SRC * CAP
PIECE = 36
BACK = 20
GATH = 2 * ROWS
PART = ROWS + 8
TP_ORDER = (10, 11, 15, 14, 13, 12, 0, 1, 2, 3, 7, 6, 5, 4, 8, 9)
TP_PLACE = tuple(TP_ORDER.index(t) for t in range(16))
LIMIT = pltpu.CompilerParams(vmem_limit_bytes=24 * 1024 * 1024)


def iota(shape, dim):
    return lax.broadcasted_iota(jnp.int32, shape, dim)


def one_if(cond):
    return jnp.where(cond, 1.0, 0.0).astype(BF)


def split_two(value):
    high = value.astype(BF)
    low = (value - high.astype(F32)).astype(BF)
    return high, low


def contract_cols(left, right):
    return lax.dot_general(left, right, (((1,), (1,)), ((), ())), preferred_element_type=F32)


def matmul(left, right):
    return lax.dot_general(left, right, (((1,), (0,)), ((), ())), preferred_element_type=F32)


def member_at(place):
    return (place + 8) & 15


def own_lanes():
    z = lax.axis_index("ep_0")
    place = (z + 8) % 16
    return (place % 4) * 32


def expand(expert, values):
    return matmul(one_if(iota((expert.shape[0], 16), 1) == expert), values)


def ranks(routes):
    count = routes.shape[1]
    expert = iota((16, count), 0)
    first = routes[0:1, :] == expert
    second = routes[1:2, :] == expert
    member = jnp.where(first | second, 1.0, 0.0)
    before = one_if(iota((count, count), 0) < iota((count, count), 1))
    rank = matmul(member.astype(BF), before)
    return first, second, member, rank


def dispatch_kernel(
    routes_hbm,
    weights_hbm,
    tokens_ref,
    grad_ref,
    gate,
    up,
    down,
    out_ref,
    swap_ref,
    data_ref,
    routes_ref,
    weights_ref,
    sems,
    move_sems,
):
    start = pl.multiple_of(lax.axis_index("tp") * 128, 128)
    small = [
        pltpu.make_async_copy(routes_hbm, routes_ref, sems.at[2]),
        pltpu.make_async_copy(weights_hbm, weights_ref, sems.at[3]),
    ]
    loads = [
        pltpu.make_async_copy(
            ref.at[:, pl.ds(start, 128)], data_ref.at[pl.ds(128 * k, 128), :], sems.at[k]
        )
        for k, ref in enumerate((tokens_ref, grad_ref))
    ]
    for load in small + loads:
        load.start()
    moves = [
        pltpu.make_async_copy(ref, swap_ref.at[pl.ds(2048 * k, 2048), :], move_sems.at[16 + k])
        for k, ref in enumerate((gate, up))
    ] + [
        pltpu.make_async_copy(
            down.at[:, pl.ds(128 * t, 128)], swap_ref.at[pl.ds(4096 + 128 * t, 128), :], move_sems.at[t]
        )
        for t in range(16)
    ]
    for move in moves:
        move.start()
    for load in small:
        load.wait()
    first, second, member, rank = ranks(routes_ref[...])
    weights = weights_ref[...]
    weight = jnp.where(first, weights[0:1, :], 0.0) + jnp.where(second, weights[1:2, :], 0.0)
    slot = jnp.where(member > 0.0, rank, -100.0)
    row = iota((16 * PIECE, 1), 0)
    place = (row * 1821) >> 16
    expert = member_at(place)
    slots = expand(expert, slot.astype(BF)).astype(jnp.int32)
    within = row - place * PIECE
    sel_x = slots == within
    sel_dy = slots + CAP == within
    high, low = split_two(weight)
    spread = expand(expert, high) + expand(expert, low)
    factor = jnp.sum(jnp.where(sel_dy, spread, 0.0), axis=1, keepdims=True)
    factor = jnp.where(within < CAP, 1.0, factor)
    chosen = jnp.concatenate([one_if(sel_x), one_if(sel_dy)], axis=1)
    for load in loads:
        load.wait()
    out_ref[...] = (matmul(chosen, data_ref[...]) * factor).astype(BF)
    for move in moves:
        move.wait()


def plan_kernel(copies_ref):
    p = iota((GATH, 1), 0)
    is_dy = p >= ROWS
    q = jnp.where(is_dy, p - ROWS, p)
    source = (q * 3641) >> 16
    target = source * PIECE + (q - source * CAP) + jnp.where(is_dy, CAP, 0)
    copies_ref[...] = one_if(iota((GATH, SRC * PIECE), 1) == target)


def places_kernel(routes_hbm, weights_hbm, combine_ref, lanes_ref, routes_ref, weights_ref, sems):
    loads = [
        pltpu.make_async_copy(routes_hbm, routes_ref, sems.at[0]),
        pltpu.make_async_copy(weights_hbm, weights_ref, sems.at[1]),
    ]
    for load in loads:
        load.start()
    for load in loads:
        load.wait()
    routes = routes_ref[...]
    first, second, member, rank = ranks(routes)
    slot = jnp.where(member > 0.0, rank, -100.0)
    row = iota((16 * BACK, 1), 0)
    place = (row * 3277) >> 16
    expert = member_at(place)
    within = row - place * BACK
    sel = jnp.where(expand(expert, slot.astype(BF)).astype(jnp.int32) == within, 1.0, 0.0)
    combine_ref[0:128, :] = jnp.transpose(sel).astype(BF)
    offset = own_lanes()
    weights = weights_ref[...]
    for k, mine in enumerate((first, second)):
        sel = jnp.where(within >= CAP, expand(expert, one_if(mine)), 0.0)
        combine_ref[128 * (k + 1) : 128 * (k + 2), :] = jnp.transpose(sel).astype(BF)
        index = jnp.sum(jnp.where(mine, rank, 0.0), axis=0, keepdims=True).astype(jnp.int32)
        lanes = jnp.where(iota((128, 128), 0) == index + offset, 1.0 / weights[k : k + 1, :], 0.0)
        lanes_ref[128 * k : 128 * (k + 1), :] = jnp.transpose(lanes)


def settle_kernel(in_ref, out_ref):
    del in_ref, out_ref


def copies_kernel(in_ref, pick_ref, out_ref):
    rows = matmul(pick_ref[...], in_ref[...]).astype(BF)
    for t in range(16):
        out_ref[t] = rows


def lane_of_row():
    r = iota((ROWS, 1), 0)
    source = (r * 3641) >> 16
    lane = (source & 3) * 32 + (r - source * CAP)
    return source >> 2, lane


def pair_cols(ref, t, start):
    return jnp.concatenate([ref[TP_PLACE[2 * t + k], start : start + ROWS, :] for k in range(2)], axis=1)


def main_kernel(own_ref, gate, up, down, swap_ref, part_out, both_ref, hidden_ref, part_ref, sems):
    pre_gate = jnp.zeros((ROWS, 256), F32)
    pre_up = jnp.zeros((ROWS, 256), F32)
    d_hidden = jnp.zeros((ROWS, 256), F32)

    def both_halves(ref, t, first):
        cols = slice(256 * t, 256 * t + 256)
        return jnp.concatenate([ref[cols, :], swap_ref[first + 256 * t : first + 256 * t + 256, :]], axis=1)

    for t in range(8):
        x = pair_cols(own_ref, t, 0)
        pre_gate = pre_gate + matmul(x, both_halves(gate, t, 0))
        pre_up = pre_up + matmul(x, both_halves(up, t, 2048))
        at = 4096 + 256 * t
        down_2 = jnp.concatenate([swap_ref[at : at + 128, :], swap_ref[at + 128 : at + 256, :]], axis=1)
        d_hidden = d_hidden + contract_cols(
            pair_cols(own_ref, t, ROWS),
            jnp.concatenate([down[:, 256 * t : 256 * t + 256], down_2], axis=0),
        )
    sigma = jax.nn.sigmoid(pre_gate)
    activ = pre_gate * sigma
    hidden = activ * pre_up
    gate_part = jnp.sum(hidden * d_hidden, axis=1, keepdims=True)
    d_gate = (d_hidden * pre_up * sigma * (1.0 + pre_gate * (1.0 - sigma))).astype(BF)
    d_up = (d_hidden * activ).astype(BF)
    both_ref[:, 0:256] = d_gate
    both_ref[:, 256:512] = d_up
    hidden_ref[...] = hidden.astype(BF)
    _, lane = lane_of_row()
    spread = jnp.where(iota((ROWS, 128), 1) == lane, gate_part, 0.0)
    packed = jnp.sum(spread.reshape(4, ROWS // 4, 128), axis=1)
    extra = jnp.concatenate(split_two(packed), axis=0)
    stores = []
    for t in range(8):
        value = contract_cols(d_gate, both_halves(gate, t, 0))
        value = value + contract_cols(d_up, both_halves(up, t, 2048))
        value = value.astype(BF)
        for k in range(2):
            place = TP_PLACE[2 * t + k]
            part_ref[place, 0:ROWS, :] = value[:, 128 * k : 128 * k + 128]
            part_ref[place, ROWS:PART, :] = extra
            stores.append(pltpu.make_async_copy(part_ref.at[place], part_out.at[place], sems.at[place]))
            stores[-1].start()
    for store in stores:
        store.wait()


def half_grads(own_ref, both_ref, hidden_ref, half):
    lanes = slice(128 * half, 128 * half + 128)
    late = slice(256 + 128 * half, 256 + 128 * half + 128)
    both = jnp.concatenate([both_ref[:, lanes], both_ref[:, late]], axis=1)
    both_t = jnp.transpose(both.astype(F32)).astype(BF)
    hidden_t = jnp.transpose(hidden_ref[:, lanes].astype(F32)).astype(BF)
    for t in range(8):
        cols = slice(256 * t, 256 * t + 256)
        grads = matmul(both_t, pair_cols(own_ref, t, 0))
        yield cols, grads, matmul(hidden_t, pair_cols(own_ref, t, ROWS))


def partner_grads_kernel(own_ref, both_ref, hidden_ref, out_ref):
    for cols, both, down in half_grads(own_ref, both_ref, hidden_ref, 1):
        out_ref[0:256, cols] = both.astype(BF)
        out_ref[256:384, cols] = down.astype(BF)


def own_grads_kernel(own_ref, both_ref, hidden_ref, other_ref, gate_out, up_out, down_out):
    for cols, both, down in half_grads(own_ref, both_ref, hidden_ref, 0):
        grads = jnp.transpose(both + other_ref[0:256, cols].astype(F32))
        gate_out[cols, :] = grads[:, :128].astype(BF)
        up_out[cols, :] = grads[:, 128:].astype(BF)
        down_out[:, cols] = (down + other_ref[256:384, cols].astype(F32)).astype(BF)


def sum_kernel(in_ref, out_ref):
    rows = in_ref[0].astype(F32)
    for t in range(1, 16):
        rows = rows + in_ref[t].astype(F32)
    packed = rows[ROWS : ROWS + 4] + rows[ROWS + 4 : PART]
    high = packed.astype(BF).astype(F32)
    rows = jnp.concatenate([rows[:ROWS], high, packed - high], axis=0).astype(BF)
    p = iota((SRC * BACK, 1), 0)
    source = (p * 3277) >> 16
    j = p - source * BACK
    target = jnp.where(j < CAP, source * CAP + j, -1)
    target = jnp.where(j == 18, ROWS + (source >> 2), target)
    target = jnp.where(j == 19, ROWS + 4 + (source >> 2), target)
    pick = one_if(iota((SRC * BACK, PART), 1) == target)
    out_ref[...] = matmul(pick, rows).astype(BF)


def combine_kernel(in_ref, pick_ref, lanes_ref, tokens_ref, route_ref):
    values = matmul(pick_ref[...], in_ref[...])
    tokens_ref[...] = values[:128].astype(BF)
    gates = lax.dot_general(
        jnp.ones((8, 128), F32),
        values[128:] * lanes_ref[...],
        (((1,), (1,)), ((), ())),
        precision=lax.Precision.HIGHEST,
        preferred_element_type=F32,
    )
    route_ref[0:1, :] = gates[0:1, :128]
    route_ref[1:2, :] = gates[0:1, 128:]


def shape(dims, dtype=BF):
    return jax.ShapeDtypeStruct(dims, dtype)


def far_shape(dims, dtype=BF):
    return pltpu.HBM(dims, dtype)


def near(dims, dtype=BF):
    return pltpu.VMEM(dims, dtype)


def far(value):
    return pltpu.with_memory_space_constraint(value, pltpu.HBM)


def hold(value):
    return pltpu.with_memory_space_constraint(value, pltpu.VMEM)


def local(tokens, routes, route_weights, out_grad, gate_proj, up_proj, down_proj):
    return steps(tokens, routes, route_weights, out_grad, gate_proj[0], up_proj[0], down_proj[0])


def exchange(value, axis):
    groups = [[(k + 8) % 16 for k in range(16)]] if axis == "ep_0" else [list(TP_ORDER)]
    return lax.all_to_all(value, axis, 0, 0, axis_index_groups=groups, tiled=True)


def to_partner(value):
    return lax.ppermute(value, "ep_1", [(0, 1), (1, 0)])


def kernel(body, **settings):
    return pl.pallas_call(body, compiler_params=LIMIT, **settings)


def steps(tokens, routes, route_weights, out_grad, gate, up, down):
    count, width = tokens.shape
    routes_t = routes.T
    weights_t = route_weights.T
    vmem = pl.BlockSpec(memory_space=pltpu.VMEM)
    hbm = pl.BlockSpec(memory_space=pltpu.HBM)
    small = [pltpu.VMEM((2, count), jnp.int32), pltpu.VMEM((2, count), F32)]
    pieces, packed = kernel(
        dispatch_kernel,
        in_specs=[hbm] * 7,
        out_specs=(vmem, vmem),
        out_shape=(near((16 * PIECE, 128)), near((3 * width, 128))),
        scratch_shapes=[
            pltpu.VMEM((256, 128), BF),
            *small,
            pltpu.SemaphoreType.DMA((4,)),
            pltpu.SemaphoreType.DMA((18,)),
        ],
    )(far(routes_t), far(weights_t), far(tokens), far(out_grad), far(gate), far(up), far(down))
    received = exchange(pieces.reshape(16, PIECE // 4, 4, 128), "ep_0")
    pick_copies = kernel(plan_kernel, out_specs=vmem, out_shape=near((GATH, SRC * PIECE)))()
    packed_2 = to_partner(packed)
    packed_2 = kernel(
        settle_kernel,
        in_specs=[hbm],
        out_specs=hbm,
        out_shape=far_shape((3 * width, 128)),
        input_output_aliases={0: 0},
    )(far(packed_2))
    copies = kernel(copies_kernel, out_shape=near((16, GATH, 128)))(
        hold(received.reshape(SRC * PIECE, 128)), hold(pick_copies)
    )
    gathered = exchange(copies, "tp")
    own, own_far = hold(gathered), far(gathered)
    part, both, hidden = kernel(
        main_kernel,
        in_specs=[vmem] * 5,
        out_specs=(hbm, vmem, vmem),
        out_shape=(far_shape((16, PART, 128)), near((ROWS, 512)), near((ROWS, 256))),
        scratch_shapes=[pltpu.VMEM((16, PART, 128), BF), pltpu.SemaphoreType.DMA((16,))],
    )(own, gate, up, down, packed_2)
    spread = exchange(part, "tp")
    partner = kernel(partner_grads_kernel, out_shape=shape((384, width)))(own_far, both, hidden)
    mine = to_partner(partner)
    gate_grad, up_grad, down_grad = kernel(
        own_grads_kernel, out_shape=(shape((width, 128)), shape((width, 128)), shape((128, width)))
    )(own_far, both, hidden, mine)
    back = kernel(sum_kernel, out_shape=near((SRC * BACK, 128)))(hold(spread))
    pick_combine, lanes = kernel(
        places_kernel,
        in_specs=[hbm] * 2,
        out_specs=(vmem, vmem),
        out_shape=(near((384, 16 * BACK)), near((256, 128), F32)),
        scratch_shapes=[*small, pltpu.SemaphoreType.DMA((2,))],
    )(far(routes_t), far(weights_t))
    home = exchange(back.reshape(SRC, BACK // 4, 4, 128), "ep_0")
    tokens_grad, route_grad = kernel(
        combine_kernel, out_shape=(shape((count, 128)), shape((2, count), F32))
    )(hold(home.reshape(16 * BACK, 128)), hold(pick_combine), hold(lanes))
    return (tokens_grad, route_grad.T, gate_grad[None], up_grad[None], down_grad[None])


def solution(mesh):
    torus = Mesh(mesh.devices.reshape(16, 2, mesh.shape["tp"]), ("ep_0", "ep_1", "tp"))
    placed = (
        P(EP, None),
        P(EP, None),
        P(EP, None),
        P(EP, None),
        P(EP, None, "tp"),
        P(EP, None, "tp"),
        P(EP, "tp", None),
    )
    return jax.shard_map(
        local,
        mesh=torus,
        in_specs=placed,
        out_specs=(
            P(EP, "tp"),
            P(EP, None),
            P(EP, None, "tp"),
            P(EP, None, "tp"),
            P(EP, "tp", None),
        ),
        check_vma=False,
    )
```

```python
import jax
import jax.numpy as jnp
from jax import lax
from jax.experimental import pallas as pl
from jax.experimental.pallas import tpu as pltpu
from jax.sharding import Mesh
from jax.sharding import PartitionSpec as P


EP = ("ep_0", "ep_1")
BF = jnp.bfloat16
F32 = jnp.float32

CAP = 18
SRC = 16
ROWS = SRC * CAP
PIECE = 36
BACK = 20
GATH = 2 * ROWS
PART = ROWS + 8
TP_ORDER = (10, 11, 15, 14, 13, 12, 0, 1, 2, 3, 7, 6, 5, 4, 8, 9)
TP_PLACE = tuple(TP_ORDER.index(t) for t in range(16))
LIMIT = pltpu.CompilerParams(vmem_limit_bytes=24 * 1024 * 1024)


def iota(shape, dim):
    return lax.broadcasted_iota(jnp.int32, shape, dim)


def one_if(cond):
    return jnp.where(cond, 1.0, 0.0).astype(BF)


def split_two(value):
    high = value.astype(BF)
    low = (value - high.astype(F32)).astype(BF)
    return high, low


def contract_cols(left, right):
    return lax.dot_general(left, right, (((1,), (1,)), ((), ())), preferred_element_type=F32)


def matmul(left, right):
    return lax.dot_general(left, right, (((1,), (0,)), ((), ())), preferred_element_type=F32)


def member_at(place):
    return (place + 10) & 15


def own_lanes():
    z = lax.axis_index("ep_0")
    place = (z + 6) % 16
    return (place % 4) * 32


def expand(expert, values):
    return matmul(one_if(iota((expert.shape[0], 16), 1) == expert), values)


def ranks(routes):
    count = routes.shape[1]
    expert = iota((16, count), 0)
    first = routes[0:1, :] == expert
    second = routes[1:2, :] == expert
    member = jnp.where(first | second, 1.0, 0.0)
    before = one_if(iota((count, count), 0) < iota((count, count), 1))
    rank = matmul(member.astype(BF), before)
    return first, second, member, rank


def dispatch_kernel(
    routes_hbm,
    weights_hbm,
    tokens_ref,
    grad_ref,
    gate,
    up,
    down,
    out_ref,
    swap_ref,
    data_ref,
    routes_ref,
    weights_ref,
    sems,
    move_sems,
):
    start = pl.multiple_of(lax.axis_index("tp") * 128, 128)
    small = [
        pltpu.make_async_copy(routes_hbm, routes_ref, sems.at[2]),
        pltpu.make_async_copy(weights_hbm, weights_ref, sems.at[3]),
    ]
    loads = [
        pltpu.make_async_copy(
            ref.at[:, pl.ds(start, 128)], data_ref.at[pl.ds(128 * k, 128), :], sems.at[k]
        )
        for k, ref in enumerate((tokens_ref, grad_ref))
    ]
    for load in small + loads:
        load.start()
    moves = [
        pltpu.make_async_copy(ref, swap_ref.at[pl.ds(2048 * k, 2048), :], move_sems.at[16 + k])
        for k, ref in enumerate((gate, up))
    ] + [
        pltpu.make_async_copy(
            down.at[:, pl.ds(128 * t, 128)], swap_ref.at[pl.ds(4096 + 128 * t, 128), :], move_sems.at[t]
        )
        for t in range(16)
    ]
    for move in moves:
        move.start()
    for load in small:
        load.wait()
    first, second, member, rank = ranks(routes_ref[...])
    weights = weights_ref[...]
    weight = jnp.where(first, weights[0:1, :], 0.0) + jnp.where(second, weights[1:2, :], 0.0)
    slot = jnp.where(member > 0.0, rank, -100.0)
    row = iota((16 * PIECE, 1), 0)
    place = (row * 1821) >> 16
    expert = member_at(place)
    slots = expand(expert, slot.astype(BF)).astype(jnp.int32)
    within = row - place * PIECE
    sel_x = slots == within
    sel_dy = slots + CAP == within
    high, low = split_two(weight)
    spread = expand(expert, high) + expand(expert, low)
    factor = jnp.sum(jnp.where(sel_dy, spread, 0.0), axis=1, keepdims=True)
    factor = jnp.where(within < CAP, 1.0, factor)
    chosen = jnp.concatenate([one_if(sel_x), one_if(sel_dy)], axis=1)
    for load in loads:
        load.wait()
    out_ref[...] = (matmul(chosen, data_ref[...]) * factor).astype(BF)
    for move in moves:
        move.wait()


def plan_kernel(copies_ref):
    p = iota((GATH, 1), 0)
    is_dy = p >= ROWS
    q = jnp.where(is_dy, p - ROWS, p)
    source = (q * 3641) >> 16
    target = source * PIECE + (q - source * CAP) + jnp.where(is_dy, CAP, 0)
    copies_ref[...] = one_if(iota((GATH, SRC * PIECE), 1) == target)


def places_kernel(routes_hbm, weights_hbm, combine_ref, lanes_ref, routes_ref, weights_ref, sems):
    loads = [
        pltpu.make_async_copy(routes_hbm, routes_ref, sems.at[0]),
        pltpu.make_async_copy(weights_hbm, weights_ref, sems.at[1]),
    ]
    for load in loads:
        load.start()
    for load in loads:
        load.wait()
    routes = routes_ref[...]
    first, second, member, rank = ranks(routes)
    slot = jnp.where(member > 0.0, rank, -100.0)
    row = iota((16 * BACK, 1), 0)
    place = (row * 3277) >> 16
    expert = member_at(place)
    within = row - place * BACK
    sel = jnp.where(expand(expert, slot.astype(BF)).astype(jnp.int32) == within, 1.0, 0.0)
    combine_ref[0:128, :] = jnp.transpose(sel).astype(BF)
    offset = own_lanes()
    weights = weights_ref[...]
    for k, mine in enumerate((first, second)):
        sel = jnp.where(within >= CAP, expand(expert, one_if(mine)), 0.0)
        combine_ref[128 * (k + 1) : 128 * (k + 2), :] = jnp.transpose(sel).astype(BF)
        index = jnp.sum(jnp.where(mine, rank, 0.0), axis=0, keepdims=True).astype(jnp.int32)
        lanes = jnp.where(iota((128, 128), 0) == index + offset, 1.0 / weights[k : k + 1, :], 0.0)
        lanes_ref[128 * k : 128 * (k + 1), :] = jnp.transpose(lanes)


def settle_kernel(in_ref, out_ref):
    del in_ref, out_ref


def copies_kernel(in_ref, pick_ref, out_ref):
    rows = matmul(pick_ref[...], in_ref[...]).astype(BF)
    for t in range(16):
        out_ref[t] = rows


def lane_of_row():
    r = iota((ROWS, 1), 0)
    source = (r * 3641) >> 16
    lane = (source & 3) * 32 + (r - source * CAP)
    return source >> 2, lane


def pair_cols(ref, t, start):
    return jnp.concatenate([ref[TP_PLACE[2 * t + k], start : start + ROWS, :] for k in range(2)], axis=1)


def main_kernel(own_ref, gate, up, down, swap_ref, part_out, both_ref, hidden_ref, part_ref, sems):
    pre_gate = jnp.zeros((ROWS, 256), F32)
    pre_up = jnp.zeros((ROWS, 256), F32)
    d_hidden = jnp.zeros((ROWS, 256), F32)

    def both_halves(ref, t, first):
        cols = slice(256 * t, 256 * t + 256)
        return jnp.concatenate([ref[cols, :], swap_ref[first + 256 * t : first + 256 * t + 256, :]], axis=1)

    for t in range(8):
        x = pair_cols(own_ref, t, 0)
        pre_gate = pre_gate + matmul(x, both_halves(gate, t, 0))
        pre_up = pre_up + matmul(x, both_halves(up, t, 2048))
        at = 4096 + 256 * t
        down_2 = jnp.concatenate([swap_ref[at : at + 128, :], swap_ref[at + 128 : at + 256, :]], axis=1)
        d_hidden = d_hidden + contract_cols(
            pair_cols(own_ref, t, ROWS),
            jnp.concatenate([down[:, 256 * t : 256 * t + 256], down_2], axis=0),
        )
    sigma = jax.nn.sigmoid(pre_gate)
    activ = pre_gate * sigma
    hidden = activ * pre_up
    gate_part = jnp.sum(hidden * d_hidden, axis=1, keepdims=True)
    d_gate = (d_hidden * pre_up * sigma * (1.0 + pre_gate * (1.0 - sigma))).astype(BF)
    d_up = (d_hidden * activ).astype(BF)
    both_ref[:, 0:256] = d_gate
    both_ref[:, 256:512] = d_up
    hidden_ref[...] = hidden.astype(BF)
    _, lane = lane_of_row()
    spread = jnp.where(iota((ROWS, 128), 1) == lane, gate_part, 0.0)
    packed = jnp.sum(spread.reshape(4, ROWS // 4, 128), axis=1)
    extra = jnp.concatenate(split_two(packed), axis=0)
    stores = []
    for t in range(8):
        value = contract_cols(d_gate, both_halves(gate, t, 0))
        value = value + contract_cols(d_up, both_halves(up, t, 2048))
        value = value.astype(BF)
        for k in range(2):
            place = TP_PLACE[2 * t + k]
            part_ref[place, 0:ROWS, :] = value[:, 128 * k : 128 * k + 128]
            part_ref[place, ROWS:PART, :] = extra
            stores.append(pltpu.make_async_copy(part_ref.at[place], part_out.at[place], sems.at[place]))
            stores[-1].start()
    for store in stores:
        store.wait()


def half_grads(own_ref, both_ref, hidden_ref, half):
    lanes = slice(128 * half, 128 * half + 128)
    late = slice(256 + 128 * half, 256 + 128 * half + 128)
    both = jnp.concatenate([both_ref[:, lanes], both_ref[:, late]], axis=1)
    both_t = jnp.transpose(both.astype(F32)).astype(BF)
    hidden_t = jnp.transpose(hidden_ref[:, lanes].astype(F32)).astype(BF)
    for t in range(8):
        cols = slice(256 * t, 256 * t + 256)
        grads = matmul(both_t, pair_cols(own_ref, t, 0))
        yield cols, grads, matmul(hidden_t, pair_cols(own_ref, t, ROWS))


def partner_grads_kernel(own_ref, both_ref, hidden_ref, out_ref):
    for cols, both, down in half_grads(own_ref, both_ref, hidden_ref, 1):
        out_ref[0:256, cols] = both.astype(BF)
        out_ref[256:384, cols] = down.astype(BF)


def own_grads_kernel(own_ref, both_ref, hidden_ref, other_ref, gate_out, up_out, down_out):
    for cols, both, down in half_grads(own_ref, both_ref, hidden_ref, 0):
        grads = jnp.transpose(both + other_ref[0:256, cols].astype(F32))
        gate_out[cols, :] = grads[:, :128].astype(BF)
        up_out[cols, :] = grads[:, 128:].astype(BF)
        down_out[:, cols] = (down + other_ref[256:384, cols].astype(F32)).astype(BF)


def sum_kernel(in_ref, out_ref):
    rows = in_ref[0].astype(F32)
    for t in range(1, 16):
        rows = rows + in_ref[t].astype(F32)
    packed = rows[ROWS : ROWS + 4] + rows[ROWS + 4 : PART]
    high = packed.astype(BF).astype(F32)
    rows = jnp.concatenate([rows[:ROWS], high, packed - high], axis=0).astype(BF)
    p = iota((SRC * BACK, 1), 0)
    source = (p * 3277) >> 16
    j = p - source * BACK
    target = jnp.where(j < CAP, source * CAP + j, -1)
    target = jnp.where(j == 18, ROWS + (source >> 2), target)
    target = jnp.where(j == 19, ROWS + 4 + (source >> 2), target)
    pick = one_if(iota((SRC * BACK, PART), 1) == target)
    out_ref[...] = matmul(pick, rows).astype(BF)


def combine_kernel(in_ref, pick_ref, lanes_ref, tokens_ref, route_ref):
    values = matmul(pick_ref[...], in_ref[...])
    tokens_ref[...] = values[:128].astype(BF)
    gates = lax.dot_general(
        jnp.ones((8, 128), F32),
        values[128:] * lanes_ref[...],
        (((1,), (1,)), ((), ())),
        precision=lax.Precision.HIGHEST,
        preferred_element_type=F32,
    )
    route_ref[0:1, :] = gates[0:1, :128]
    route_ref[1:2, :] = gates[0:1, 128:]


def shape(dims, dtype=BF):
    return jax.ShapeDtypeStruct(dims, dtype)


def far_shape(dims, dtype=BF):
    return pltpu.HBM(dims, dtype)


def near(dims, dtype=BF):
    return pltpu.VMEM(dims, dtype)


def far(value):
    return pltpu.with_memory_space_constraint(value, pltpu.HBM)


def hold(value):
    return pltpu.with_memory_space_constraint(value, pltpu.VMEM)


def local(tokens, routes, route_weights, out_grad, gate_proj, up_proj, down_proj):
    return steps(tokens, routes, route_weights, out_grad, gate_proj[0], up_proj[0], down_proj[0])


def exchange(value, axis):
    groups = [[(k + 10) % 16 for k in range(16)]] if axis == "ep_0" else [list(TP_ORDER)]
    return lax.all_to_all(value, axis, 0, 0, axis_index_groups=groups, tiled=True)


def to_partner(value):
    return lax.ppermute(value, "ep_1", [(0, 1), (1, 0)])


def kernel(body, **settings):
    return pl.pallas_call(body, compiler_params=LIMIT, **settings)


def steps(tokens, routes, route_weights, out_grad, gate, up, down):
    count, width = tokens.shape
    routes_t = routes.T
    weights_t = route_weights.T
    vmem = pl.BlockSpec(memory_space=pltpu.VMEM)
    hbm = pl.BlockSpec(memory_space=pltpu.HBM)
    small = [pltpu.VMEM((2, count), jnp.int32), pltpu.VMEM((2, count), F32)]
    pieces, packed = kernel(
        dispatch_kernel,
        in_specs=[hbm] * 7,
        out_specs=(vmem, vmem),
        out_shape=(near((16 * PIECE, 128)), near((3 * width, 128))),
        scratch_shapes=[
            pltpu.VMEM((256, 128), BF),
            *small,
            pltpu.SemaphoreType.DMA((4,)),
            pltpu.SemaphoreType.DMA((18,)),
        ],
    )(far(routes_t), far(weights_t), far(tokens), far(out_grad), far(gate), far(up), far(down))
    received = exchange(pieces.reshape(16, PIECE // 4, 4, 128), "ep_0")
    pick_copies = kernel(plan_kernel, out_specs=vmem, out_shape=near((GATH, SRC * PIECE)))()
    packed_2 = to_partner(packed)
    packed_2 = kernel(
        settle_kernel,
        in_specs=[hbm],
        out_specs=hbm,
        out_shape=far_shape((3 * width, 128)),
        input_output_aliases={0: 0},
    )(far(packed_2))
    copies = kernel(copies_kernel, out_shape=near((16, GATH, 128)))(
        hold(received.reshape(SRC * PIECE, 128)), hold(pick_copies)
    )
    gathered = exchange(copies, "tp")
    own, own_far = hold(gathered), far(gathered)
    part, both, hidden = kernel(
        main_kernel,
        in_specs=[vmem] * 5,
        out_specs=(hbm, vmem, vmem),
        out_shape=(far_shape((16, PART, 128)), near((ROWS, 512)), near((ROWS, 256))),
        scratch_shapes=[pltpu.VMEM((16, PART, 128), BF), pltpu.SemaphoreType.DMA((16,))],
    )(own, gate, up, down, packed_2)
    spread = exchange(part, "tp")
    partner = kernel(partner_grads_kernel, out_shape=shape((384, width)))(own_far, both, hidden)
    mine = to_partner(partner)
    gate_grad, up_grad, down_grad = kernel(
        own_grads_kernel, out_shape=(shape((width, 128)), shape((width, 128)), shape((128, width)))
    )(own_far, both, hidden, mine)
    back = kernel(sum_kernel, out_shape=near((SRC * BACK, 128)))(hold(spread))
    pick_combine, lanes = kernel(
        places_kernel,
        in_specs=[hbm] * 2,
        out_specs=(vmem, vmem),
        out_shape=(near((384, 16 * BACK)), near((256, 128), F32)),
        scratch_shapes=[*small, pltpu.SemaphoreType.DMA((2,))],
    )(far(routes_t), far(weights_t))
    home = exchange(back.reshape(SRC, BACK // 4, 4, 128), "ep_0")
    tokens_grad, route_grad = kernel(
        combine_kernel, out_shape=(shape((count, 128)), shape((2, count), F32))
    )(hold(home.reshape(16 * BACK, 128)), hold(pick_combine), hold(lanes))
    return (tokens_grad, route_grad.T, gate_grad[None], up_grad[None], down_grad[None])


def solution(mesh):
    torus = Mesh(mesh.devices.reshape(16, 2, mesh.shape["tp"]), ("ep_0", "ep_1", "tp"))
    placed = (
        P(EP, None),
        P(EP, None),
        P(EP, None),
        P(EP, None),
        P(EP, None, "tp"),
        P(EP, None, "tp"),
        P(EP, "tp", None),
    )
    return jax.shard_map(
        local,
        mesh=torus,
        in_specs=placed,
        out_specs=(
            P(EP, "tp"),
            P(EP, None),
            P(EP, None, "tp"),
            P(EP, None, "tp"),
            P(EP, "tp", None),
        ),
        check_vma=False,
    )
```
